128 devices in a mesh: ep: 128 (over z, y, x, core).
Axes of the slice: x: 4, y: 4, z: 4, core: 2. Of those that a mesh axis runs over, the one named last changes fastest.
Arguments:
- tokens: bfloat16 [512, 4, 1024], P('ep'), may hold values from -6 to 6
- lengths: int32 [512], P('ep'), may hold values from 1 to 4, 768 in all
- routes: int32 [512, 4, 8], P('ep'), may hold values from 0 to 255, all different within a row; in each aligned block of 16 rows (0 to 15, 16 to 31, ...) at most 4 rows name the same one
- gates: float32 [512, 4, 8], P('ep'), may hold values from 0.05 to 0.6
- norm_gain: float32 [1024], replicated, may hold values from 0.5 to 1.5
- expert_gate: bfloat16 [256, 1024, 256], P('ep'), may hold values from -0.1875 to 0.1875
- expert_up: bfloat16 [256, 1024, 256], P('ep'), may hold values from -0.1875 to 0.1875
- expert_down: bfloat16 [256, 256, 1024], P('ep'), may hold values from -0.375 to 0.375
- shared_gate: bfloat16 [1024, 256], replicated, may hold values from -0.1875 to 0.1875
- shared_up: bfloat16 [1024, 256], replicated, may hold values from -0.1875 to 0.1875
- shared_down: bfloat16 [256, 1024], replicated, may hold values from -0.375 to 0.375
- out_gain: float32 [1024], replicated, may hold values from 0.5 to 1.5
Outputs:
- mixed: bfloat16 [512, 4, 1024], P('ep')
The draws below stay inside these ranges and needn't reach their ends.
Inputs may be any that keep to these rules, and one draw needn't show every extreme that they name: `routes`: in the 16 rows of one device (all slots, in order), no expert is named by more than 4 rows, and some device reaches 4; the experts of one row differ. `lengths`: each sequence has 1 to 4 live slots, the longest exactly 4.
All inputs are finite; a program needn't handle non-finite values.
Results may differ from the reference program's by a relative error of at most 0.0065.
Values may be sent and summed in bfloat16 or wider, within the bound.
No kernel may reach another device: no remote copies, remote signals or barrier semaphores. Data moves between devices by JAX's collectives and lax.ppermute only.
A program may use at most 64 MiB of HBM per device.

```python
import math
import jax
import jax.numpy as jnp
import numpy as np
from jax import lax

D = 1024
FF = 256
SFF = 256
TOP = 8
NEW = 4
MOST = 4
SEQUENCES = 512
TOK_DEV = 16
EXPERTS = 256


def block_scale(rng, shape, split, smallest, high):
    factor_of, own = 1.0, jax.random.fold_in(rng, 6)
    for position, parts in split:
        heights = jnp.exp(jax.random.uniform(jax.random.fold_in(own, position), (parts,), jnp.float32, smallest / len(split), high / len(split)))
        factor_of = factor_of * jnp.repeat(heights, shape[position] // parts).reshape([-1 if axis == position else 1 for axis in range(len(shape))])
    return factor_of


def length_profile(number_of, total, most, skew):
    portions = [(1 << 20) // math.isqrt(rank ** skew) + 1 for rank in range(2, number_of + 1)]
    surplus, given = total - most - (number_of - 1), [1] * (number_of - 1)
    while surplus > 0:
        free = [i for i in range(number_of - 1) if given[i] < most]
        whole, remaining = sum([portions[i] for i in free]), surplus
        for i in free:
            addition = min(most - given[i], max(1, remaining * portions[i] // whole), surplus)
            given[i] = given[i] + addition
            surplus = surplus - addition
    return np.array([most] + given)


def uneven(rng, amount, total, most, lean):
    if amount == 2:
        one = jax.random.randint(rng, (), max(1, total - most), min(most, total - 1) + 1)
        return jnp.stack([one, total - one])
    sizes = jnp.asarray(length_profile(amount, total, most, lean), jnp.int32)
    twos = (amount - 1) // 2
    donor, sink = sizes[1:1 + 2 * twos:2], sizes[2:2 + 2 * twos:2]
    slack = jnp.minimum(donor - 1, most - sink)
    passed = jax.random.randint(jax.random.fold_in(rng, 1), (twos,), 0, 1 << 20) % (slack + 1)
    sizes = sizes.at[1:1 + 2 * twos:2].set(donor - passed).at[2:2 + 2 * twos:2].set(sink + passed)
    return sizes[jax.random.permutation(jax.random.fold_in(rng, 2), amount)]


def shared_out(key, own, number, rows, number_of, top, limit, slope):
    sequence = jax.random.permutation(key, number_of)
    heavy_load, usual = portions_of(number_of, rows * top, limit, slope, True), portions_of(number_of, rows * top, limit, slope, False)
    places = jnp.arange(number_of)

    def named(sizes, rotation):
        used = int((sizes > 0).sum())
        fixed = max(1, used // 4)
        passed = fixed + (places - fixed + rotation * (used - fixed)) % max(1, number_of - fixed)
        return jnp.zeros((number_of,), jnp.int32).at[sequence[jnp.where(places < fixed, places, passed)]].set(jnp.asarray(sizes, jnp.int32))

    sizes = jnp.where(number % 4 == 0, named(heavy_load, number // 4), named(usual, number - number // 4 - 1))
    mixed = jax.random.permutation(jax.random.fold_in(own, 3), number_of)
    donor, sink = mixed[0:number_of // 2 * 2:2], mixed[1:number_of // 2 * 2:2]
    room = jnp.minimum(sizes[donor] - 1, limit - sizes[sink]) // 2
    room = jnp.where((donor == sequence[0]) | (sink == sequence[0]) | (sizes[sink] == 0), 0, jnp.maximum(room, 0))
    passed = jax.random.randint(jax.random.fold_in(own, 4), (number_of // 2,), 0, 1 << 20) % (room + 1)
    sizes = sizes.at[donor].add(-passed).at[sink].add(passed)
    members = jnp.searchsorted(jnp.cumsum(sizes), jnp.arange(rows * top), side="right").astype(jnp.int32)
    grid = members.reshape(top, rows).T
    grid = grid[jax.random.permutation(jax.random.fold_in(own, 1), rows)]
    rotation = jax.random.randint(jax.random.fold_in(own, 2), (rows, 1), 0, top)
    return jnp.take_along_axis(grid, (jnp.arange(top)[None, :] + rotation) % top, axis=1)


def portions_of(number_of, total, limit, lean, full):
    portions = [(1 << 20) // math.isqrt(standing ** lean) + 1 for standing in range(1, number_of + 1)]
    largest = limit if full else min(limit, max(-(-total // number_of), total * portions[0] // sum(portions)))
    least = 1 if total - largest >= number_of - 1 else 0
    holding, rest = [largest] + [least] * (number_of - 1), total - largest - least * (number_of - 1)
    while rest > 0:
        free = [i for i in range(1, number_of) if holding[i] < largest] or [i for i in range(1, number_of) if holding[i] < limit]
        whole, budget = sum([portions[i] for i in free]), rest
        for i in free:
            addition = min(limit - holding[i], max(1, budget * portions[i] // whole), rest)
            holding[i] = holding[i] + addition
            rest = rest - addition
    return np.array(holding)


def centred(own_key, shape, spread, bound, shards=(), kind=jnp.bfloat16):
    entries = jax.random.normal(own_key, shape, jnp.float32) * spread
    if len(shards) > 0:
        entries = block_scale(own_key, shape, shards, -0.22, 0.18) * entries
    return jnp.clip(entries, min=-bound, max=bound).astype(kind)


def setup_inputs(seed: int = 0) -> dict:
    streams_of = jax.random.split(jax.random.key(seed), 13)
    tokens = centred(streams_of[0], (SEQUENCES, NEW, D), 1.0, 6.0, ((0, 128),))
    lengths = uneven(streams_of[1], SEQUENCES, SEQUENCES * 3 // 2, NEW, 2).astype(jnp.int32)
    routes_keys = jax.random.split(jax.random.fold_in(streams_of[2], 1), SEQUENCES * NEW // TOK_DEV)
    routes_turns = jax.random.permutation(jax.random.fold_in(streams_of[2], 3), SEQUENCES * NEW // TOK_DEV)
    routes = jax.vmap(lambda own, number: shared_out(jax.random.fold_in(streams_of[2], 2), own, number, TOK_DEV, EXPERTS, TOP, MOST, 2))(routes_keys, routes_turns).reshape((SEQUENCES, NEW, TOP))
    gates = jnp.clip(0.05 + 0.55 * jax.random.uniform(streams_of[3], (SEQUENCES, NEW, TOP), jnp.float32) ** block_scale(streams_of[3], (SEQUENCES, NEW, TOP), ((0, 128),), -0.2, 0.2), 0.05, 0.6)
    norm_gain = jnp.clip(1.0 + 0.1 * jax.random.normal(streams_of[4], (D,), jnp.float32), 0.5, 1.5)
    expert_gate = centred(streams_of[5], (EXPERTS, D, FF), D ** -0.5, 0.1875, ((0, 128),))
    expert_up = centred(streams_of[6], (EXPERTS, D, FF), D ** -0.5, 0.1875, ((0, 128),))
    expert_down = centred(streams_of[7], (EXPERTS, FF, D), FF ** -0.5, 0.375, ((0, 128),))
    shared_gate = centred(streams_of[8], (D, SFF), D ** -0.5, 0.1875)
    shared_up = centred(streams_of[9], (D, SFF), D ** -0.5, 0.1875)
    shared_down = centred(streams_of[10], (SFF, D), SFF ** -0.5, 0.375)
    out_gain = jnp.clip(1.0 + 0.1 * jax.random.normal(streams_of[11], (D,), jnp.float32), 0.5, 1.5)
    return {"tokens": tokens, "lengths": lengths, "routes": routes, "gates": gates, "norm_gain": norm_gain, "expert_gate": expert_gate, "expert_up": expert_up, "expert_down": expert_down, "shared_gate": shared_gate, "shared_up": shared_up, "shared_down": shared_down, "out_gain": out_gain}


EPS = 1e-06

def norm_rows(values, scales):
    wide = values.astype(jnp.float32)
    return wide * lax.rsqrt(lax.optimization_barrier(jnp.mean(wide * wide, axis=-1, keepdims=True)) + EPS) * scales

def reference(tokens, lengths, routes, gates, norm_gain, expert_gate, expert_up, expert_down, shared_gate, shared_up, shared_down, out_gain):
    features = tokens.shape[-1]
    flat_rows = tokens.reshape(-1, features)
    normed = norm_rows(flat_rows, norm_gain).astype(jnp.bfloat16)
    live_mask = (jnp.arange(NEW, dtype=jnp.int32)[None, :] < lengths[:, None]).reshape(-1)
    expert_ids = routes.reshape(-1)
    copies = jnp.repeat(normed, TOP, axis=0)
    block_rows = 32
    row_blocks = copies.reshape(-1, block_rows, features)
    id_blocks = expert_ids.reshape(-1, block_rows)

    def one_block(pair):
        rows_in, ids_in = pair
        wide_rows = rows_in.astype(jnp.float32)
        gate_part = jnp.einsum('rd,rdf->rf', wide_rows, expert_gate[ids_in].astype(jnp.float32))
        up_part = jnp.einsum('rd,rdf->rf', wide_rows, expert_up[ids_in].astype(jnp.float32))
        hidden = (jax.nn.silu(gate_part) * up_part).astype(jnp.bfloat16)
        result = jnp.einsum('rf,rfd->rd', hidden.astype(jnp.float32), expert_down[ids_in].astype(jnp.float32))
        return result.astype(jnp.bfloat16)
    outputs = lax.map(one_block, (row_blocks, id_blocks)).reshape(-1, TOP, features)
    weights = jnp.where(live_mask[:, None], gates.reshape(-1, TOP), jnp.float32(0.0))
    routed = lax.optimization_barrier(jnp.sum(weights[:, :, None] * outputs.astype(jnp.float32), axis=1))
    shared_hidden = (jax.nn.silu(jnp.dot(normed, shared_gate, preferred_element_type=jnp.float32)) * jnp.dot(normed, shared_up, preferred_element_type=jnp.float32)).astype(jnp.bfloat16)
    shared = jnp.dot(shared_hidden, shared_down, preferred_element_type=jnp.float32)
    summed = routed + shared
    mixed_out = jnp.where(live_mask[:, None], norm_rows(summed, out_gain), jnp.float32(0.0))
    return mixed_out.astype(jnp.bfloat16).reshape(tokens.shape)
```

```python
import functools

import jax
import jax.numpy as jnp
from jax import lax
from jax.experimental import pallas as pl
from jax.experimental.pallas import tpu as pltpu
from jax.sharding import PartitionSpec as P

MOST = 4
EPS = 1e-06
SLOTS = 8
ROWS = SLOTS - 1
FLAG_LANE = 64
BLOCK = 64

f32 = jnp.float32
bf16 = jnp.bfloat16
i32 = jnp.int32


def norm_rows(values, scales):
    wide = values.astype(jnp.float32)
    return wide * lax.rsqrt(jnp.mean(wide * wide, axis=-1, keepdims=True) + EPS) * scales


def run_experts(stacked, expert_gate, expert_up, expert_down):
    gate_part = jnp.einsum("erd,edf->erf", stacked, expert_gate, preferred_element_type=jnp.float32)
    up_part = jnp.einsum("erd,edf->erf", stacked, expert_up, preferred_element_type=jnp.float32)
    hidden = (jax.nn.silu(gate_part) * up_part).astype(jnp.bfloat16)
    return jnp.einsum(
        "erf,efd->erd", hidden, expert_down, preferred_element_type=jnp.float32
    ).astype(jnp.bfloat16)


def padded_path(normed, expert_ids, live_mask, weights, expert_gate, expert_up, expert_down):
    token_count, top_count = expert_ids.shape
    features = normed.shape[1]
    local_count = expert_gate.shape[0]
    devices = lax.axis_size("ep")
    experts_all = local_count * devices
    flat_ids = expert_ids.reshape(-1)
    live_rows = jnp.repeat(live_mask, top_count)
    matches = (
        (flat_ids[:, None] == lax.broadcasted_iota(jnp.int32, (1, experts_all), 1))
        & live_rows[:, None]
    ).astype(jnp.int32)
    earlier = jnp.cumsum(matches, axis=0) - matches
    position = jnp.sum(earlier * matches, axis=1)
    targets = jnp.where(live_rows, flat_ids * MOST + position, experts_all * MOST)
    copies = jnp.repeat(normed, top_count, axis=0)
    outgoing = (
        jnp.zeros((experts_all * MOST, features), jnp.bfloat16).at[targets].set(copies, mode="drop")
    )
    outgoing = outgoing.reshape(devices, local_count * MOST, features)
    arrived = lax.all_to_all(outgoing, "ep", split_axis=0, concat_axis=0, tiled=True)
    stacked = (
        arrived.reshape(devices, local_count, MOST, features)
        .transpose(1, 0, 2, 3)
        .reshape(local_count, devices * MOST, features)
    )
    results = run_experts(stacked, expert_gate, expert_up, expert_down)
    replies = (
        results.reshape(local_count, devices, MOST, features)
        .transpose(1, 0, 2, 3)
        .reshape(devices, local_count * MOST, features)
    )
    returned = lax.all_to_all(replies, "ep", split_axis=0, concat_axis=0, tiled=True)
    returned_flat = returned.reshape(experts_all * MOST, features)
    fetched = returned_flat[jnp.minimum(targets, experts_all * MOST - 1)].reshape(
        token_count, top_count, features
    )
    return jnp.sum(weights[:, :, None] * fetched.astype(jnp.float32), axis=1)


def iota(shape, dim):
    return lax.broadcasted_iota(i32, shape, dim)


def dot(a, b):
    return jnp.dot(a, b, preferred_element_type=f32)


def one_hot(mask):
    return jnp.where(mask, 1.0, 0.0).astype(bf16)


def spread(columns, top):
    rows = columns.shape[0]
    return jnp.concatenate(
        [jnp.broadcast_to(columns[:, k : k + 1], (rows, 128)) for k in range(top)], axis=0
    )


def dispatch_kernel(
    core_ref, len_own, len_sib, tok_own, tok_sib, rt_own, rt_sib, gt_own, gt_sib, gain_ref,
    send_ref, aux_ref, normed_ref, x_s, r_s, g_s,
):
    core = core_ref[0]
    first = core == 0
    seqs, new, features = tok_own.shape
    rows = seqs * new
    top = rt_own.shape[2]
    pairs = 2 * rows * top
    slots_all = send_ref.shape[0]
    for half, (tok, rt, gt) in enumerate(((tok_own, rt_own, gt_own), (tok_sib, rt_sib, gt_sib))):
        for i in range(seqs):
            at = half * rows + i * new
            x_s[at : at + new, :] = tok[i].astype(f32)
            r_s[at : at + new, :] = rt[i]
            g_s[at : at + new, :] = gt[i]

    def ordered(full):
        own, sib = full[:rows], full[rows:]
        return jnp.concatenate([jnp.where(first, own, sib), jnp.where(first, sib, own)], axis=0)

    wide = x_s[...]
    normed = wide * lax.rsqrt(jnp.mean(wide * wide, axis=-1, keepdims=True) + EPS) * gain_ref[...]
    normed_ref[...] = normed[:rows].astype(bf16)
    both = ordered(normed).astype(bf16)
    copies = jnp.concatenate([both] * top, axis=0)

    token = iota((2 * rows, 128), 0)
    length = jnp.zeros((2 * rows, 128), i32)
    for s in range(2 * seqs):
        low, high = (len_own, len_sib) if s < seqs else (len_sib, len_own)
        value = jnp.where(first, low[s % seqs], high[s % seqs])
        length = jnp.where(token // new == s, value, length)
    live_token = jnp.where(token % new < length, 1, 0)
    live = jnp.concatenate([live_token] * top, axis=0) > 0
    expert = spread(ordered(r_s[...]), top)
    gate = spread(ordered(g_s[...]), top)

    chip = jnp.where(live, expert >> 2, -1).astype(f32)
    local = (expert & 3).astype(f32)
    chip_wide = jnp.concatenate([chip] * (pairs // 128), axis=1)
    i0, i1 = iota((pairs, pairs), 0), iota((pairs, pairs), 1)
    chip_row = jnp.sum(jnp.where(i0 == i1, chip_wide, 0.0), axis=0, keepdims=True)
    equal = chip_wide == chip_row
    pos_row = jnp.sum(jnp.where(equal & (i0 < i1), 1.0, 0.0), axis=0, keepdims=True).astype(i32)
    pos_col = jnp.sum(jnp.where(equal & (i1 < i0), 1.0, 0.0), axis=1, keepdims=True).astype(i32)

    def placed(where_to, pos):
        chip_i = where_to.astype(i32)
        slot = pos >> 1
        live_here = chip_i >= 0
        mine = live_here & ((pos & 1) == core) & (slot < ROWS)
        target = jnp.where(mine, chip_i * SLOTS + slot, -1)
        return target, slot, mine, live_here & (slot >= ROWS)

    target_row, _, _, over_row = placed(chip_row, pos_row)
    target_col, slot_col, mine_col, over_col = placed(chip, jnp.broadcast_to(pos_col, chip.shape))

    lane = iota((pairs, 128), 1)
    labels = jnp.where(
        over_col,
        jnp.where(lane == FLAG_LANE, 1.0, 0.0),
        jnp.where(mine_col & (lane == slot_col), local + 1.0, 0.0),
    ).astype(bf16)
    aux_ref[...] = jnp.where(lane == 0, target_col.astype(f32), jnp.where(lane == 1, gate, 0.0))

    over_row_i = jnp.where(over_row, 1, 0)
    home_row = jnp.where(target_row >= 0, target_row >> 3, -1)
    step = 128
    for base in range(0, slots_all, step):
        slot_id = iota((step, pairs), 0) + base
        picks = one_hot(slot_id == target_row)
        marks = one_hot(
            ((slot_id & (SLOTS - 1)) == ROWS) & (((slot_id >> 3) == home_row) | (over_row_i > 0))
        )
        main = dot(picks, copies)
        meta = dot(marks, labels)
        send_ref[base : base + step, 128:] = main[:, 128:].astype(bf16)
        send_ref[base : base + step, :128] = (main[:, :128] + meta).astype(bf16)


def expert_kernel(
    core_ref, arrived_ref, gate_own, gate_sib, up_own, up_sib, down_own, down_sib,
    reply_ref, flag_ref, wg, wu, wd, x_s, o_s, sems,
):
    core = core_ref[0]
    own = gate_own.shape[0]
    copies = []
    for i, (src, dst, at) in enumerate(
        (
            (gate_own, wg, 0), (up_own, wu, 0), (down_own, wd, 0),
            (gate_sib, wg, own), (up_sib, wu, own), (down_sib, wd, own),
        )
    ):
        copy = pltpu.make_async_copy(src, dst.at[pl.ds(at, own)], sems.at[i])
        copy.start()
        copies.append(copy)
    slots_all = arrived_ref.shape[0]
    messages = slots_all // SLOTS
    x_s[...] = jnp.zeros_like(x_s)
    o_s[...] = jnp.zeros_like(o_s)

    pick_meta = one_hot(iota((messages, slots_all), 1) == iota((messages, slots_all), 0) * SLOTS + ROWS)
    meta = dot(pick_meta, arrived_ref[:, :128])
    flag = jnp.sum(jnp.where(iota(meta.shape, 1) == FLAG_LANE, meta, 0.0))
    flag_ref[0] = jnp.where(flag > 0.0, 1, 0)
    s_lane, s_row = iota((128, slots_all), 1), iota((128, slots_all), 0)
    expand = one_hot(((s_lane & (SLOTS - 1)) == s_row) & (s_row < ROWS))
    ids = dot(meta.astype(bf16), expand)
    message, slot = iota((messages, slots_all), 0), iota((messages, slots_all), 1)
    ids = jnp.sum(jnp.where((slot >> 3) == message, ids, 0.0), axis=0, keepdims=True).astype(i32)
    which = jnp.where(ids > 0, (ids - 1 + own * core) & (2 * own - 1), -1)
    hot = one_hot(iota((SLOTS, slots_all), 0) == which)
    earlier = one_hot(iota((slots_all, slots_all), 0) < iota((slots_all, slots_all), 1))
    rank = dot(hot, earlier).astype(i32)
    place = jnp.full((1, slots_all), -1, i32)
    start = jnp.int32(0)
    spans = []
    for j in range(2 * own):
        count = jnp.sum(jnp.where(which == j, 1.0, 0.0)).astype(i32)
        place = jnp.where(which == j, rank[j : j + 1] + start, place)
        spans.append((start, count))
        start = start + ((count + 15) // 16) * 16
    total = start

    def gather(b, carry):
        base = pl.multiple_of(b * 128, 128)
        picks = one_hot(iota((128, slots_all), 0) + base == place)
        x_s[pl.ds(base, 128), :] = dot(picks, arrived_ref[...]).astype(bf16)
        return carry

    lax.fori_loop(0, (total + 127) // 128, gather, 0)

    for j, (begin, count) in enumerate(spans):
        if j == 0:
            for copy in copies[:3]:
                copy.wait()
        if j == own:
            for copy in copies[3:]:
                copy.wait()

        def block(b, carry, j=j, begin=begin):
            base = pl.multiple_of(begin + b * BLOCK, 16)
            x = x_s[pl.ds(base, BLOCK), :]
            gate_part = dot(x, wg[j])
            up_part = dot(x, wu[j])
            hidden = (gate_part / (1.0 + jnp.exp(-gate_part)) * up_part).astype(bf16)
            o_s[pl.ds(base, BLOCK), :] = dot(hidden, wd[j]).astype(bf16)
            return carry

        lax.fori_loop(0, (count + BLOCK - 1) // BLOCK, block, 0)

    def scatter(depth):
        for base in range(0, slots_all, 128):
            same = iota((128, slots_all), 0) + base == iota((128, slots_all), 1)
            place_f = place.astype(f32)
            column = jnp.sum(jnp.where(same, place_f, 0.0), axis=1, keepdims=True).astype(i32)
            picks = one_hot(iota((128, depth), 1) == column)
            reply_ref[base : base + 128, :] = dot(picks, o_s[:depth, :]).astype(bf16)

    @pl.when(total <= 256)
    def _():
        scatter(256)

    @pl.when(total > 256)
    def _():
        scatter(512)


def combine_kernel(core_ref, returned_ref, aux_ref, own_ref, sib_ref):
    first = core_ref[0] == 0
    pairs = aux_ref.shape[0]
    slots_all = returned_ref.shape[0]
    rows = own_ref.shape[0]
    target = aux_ref[:, 0:1].astype(i32)
    gate = aux_ref[:, 1:2]
    total = jnp.zeros((2 * rows, returned_ref.shape[1]), f32)
    step = 128
    for base in range(0, pairs, step):
        picks = one_hot(iota((step, slots_all), 1) == target[base : base + step])
        fetched = dot(picks, returned_ref[...])
        weighted = fetched * gate[base : base + step]
        for k in range(0, step, 2 * rows):
            total = total + weighted[k : k + 2 * rows]
    low, high = total[:rows], total[rows:]
    own_ref[...] = jnp.where(first, low, high)
    sib_ref[...] = jnp.where(first, high, low)


def shared_kernel(normed_ref, gate_ref, up_ref, down_ref, out_ref):
    normed = normed_ref[...]
    gate_part = dot(normed, gate_ref[...])
    up_part = dot(normed, up_ref[...])
    hidden = (gate_part / (1.0 + jnp.exp(-gate_part)) * up_part).astype(bf16)
    out_ref[...] = dot(hidden, down_ref[...])


def final_kernel(len_ref, routed_ref, shared_ref, gain_ref, out_ref):
    seqs, new, features = out_ref.shape
    summed = routed_ref[...] + shared_ref[...]
    mixed = summed * lax.rsqrt(jnp.mean(summed * summed, axis=-1, keepdims=True) + EPS) * gain_ref[...]
    for s in range(seqs):
        live = iota((new, features), 0) < len_ref[s]
        out_ref[s] = jnp.where(live, mixed[s * new : (s + 1) * new], 0.0).astype(bf16)


VMEM = pl.BlockSpec(memory_space=pltpu.VMEM)
SMEM = pl.BlockSpec(memory_space=pltpu.SMEM)
HBM = pl.BlockSpec(memory_space=pltpu.HBM)


def per_device(
    tokens, lengths, routes, gates, norm_gain, expert_gate, expert_up, expert_down,
    shared_gate, shared_up, shared_down, out_gain,
):
    seqs, new, features = tokens.shape
    rows = seqs * new
    top = routes.shape[2]
    hidden = expert_gate.shape[2]
    own = expert_gate.shape[0]
    devices = lax.axis_size("ep")
    chips = devices // 2
    slots_all = chips * SLOTS
    pairs = 2 * rows * top
    core = (lax.axis_index("ep") & 1).astype(i32).reshape(1)
    swap = [(d, d ^ 1) for d in range(devices)]
    groups = [[2 * c + k for c in range(chips)] for k in range(2)]
    sibling = functools.partial(lax.ppermute, axis_name="ep", perm=swap)

    tok_sib, len_sib, rt_sib, gt_sib = (sibling(v) for v in (tokens, lengths, routes, gates))
    gate_sib, up_sib, down_sib = (sibling(v) for v in (expert_gate, expert_up, expert_down))

    send, aux, normed = pl.pallas_call(
        dispatch_kernel,
        out_shape=(
            jax.ShapeDtypeStruct((slots_all, features), bf16),
            jax.ShapeDtypeStruct((pairs, 128), f32),
            jax.ShapeDtypeStruct((rows, features), bf16),
        ),
        in_specs=[SMEM] * 3 + [VMEM] * 7,
        out_specs=(VMEM, VMEM, VMEM),
        scratch_shapes=[
            pltpu.VMEM((2 * rows, features), f32),
            pltpu.VMEM((2 * rows, top), i32),
            pltpu.VMEM((2 * rows, top), f32),
        ],
        name="dispatch",
    )(
        core, lengths, len_sib, tokens, tok_sib, routes, rt_sib, gates, gt_sib,
        norm_gain.reshape(1, features),
    )

    def exchange(values):
        return lax.all_to_all(
            values.reshape(chips, SLOTS, features), "ep", split_axis=0, concat_axis=0,
            axis_index_groups=groups, tiled=True,
        ).reshape(slots_all, features)

    arrived = exchange(send)
    replies, flag = pl.pallas_call(
        expert_kernel,
        out_shape=(
            jax.ShapeDtypeStruct((slots_all, features), bf16),
            jax.ShapeDtypeStruct((1,), i32),
        ),
        in_specs=[SMEM, VMEM] + [HBM] * 6,
        out_specs=(VMEM, SMEM),
        scratch_shapes=[
            pltpu.VMEM((2 * own, features, hidden), bf16),
            pltpu.VMEM((2 * own, features, hidden), bf16),
            pltpu.VMEM((2 * own, hidden, features), bf16),
            pltpu.VMEM((slots_all + 128, features), bf16),
            pltpu.VMEM((slots_all + 128, features), bf16),
            pltpu.SemaphoreType.DMA((6,)),
        ],
        name="experts",
    )(core, arrived, expert_gate, gate_sib, expert_up, up_sib, expert_down, down_sib)

    shared = pl.pallas_call(
        shared_kernel,
        out_shape=jax.ShapeDtypeStruct((rows, features), f32),
        in_specs=[VMEM] * 4,
        out_specs=VMEM,
        name="shared",
    )(normed, shared_gate, shared_up, shared_down)

    def short_way(replies):
        returned = exchange(replies)
        mine, other = pl.pallas_call(
            combine_kernel,
            out_shape=(jax.ShapeDtypeStruct((rows, features), f32),) * 2,
            in_specs=[SMEM, VMEM, VMEM],
            out_specs=(VMEM, VMEM),
            name="combine",
        )(core, returned, aux)
        return mine + sibling(other)

    def long_way(replies):
        live_mask = (lax.broadcasted_iota(i32, (seqs, new), 1) < lengths[:, None]).reshape(-1)
        expert_ids = routes.reshape(rows, top)
        weights = jnp.where(live_mask[:, None], gates.reshape(rows, top), 0.0)
        return padded_path(
            normed, expert_ids, live_mask, weights, expert_gate, expert_up, expert_down
        )

    routed = lax.cond(flag[0] > 0, long_way, short_way, replies)
    return pl.pallas_call(
        final_kernel,
        out_shape=jax.ShapeDtypeStruct(tokens.shape, bf16),
        in_specs=[SMEM] + [VMEM] * 3,
        out_specs=VMEM,
        name="final",
    )(lengths, routed, shared, out_gain.reshape(1, features))


def solution(mesh):
    placed = (
        P("ep", None, None),
        P("ep"),
        P("ep", None, None),
        P("ep", None, None),
        P(),
        P("ep", None, None),
        P("ep", None, None),
        P("ep", None, None),
        P(),
        P(),
        P(),
        P(),
    )
    return jax.shard_map(
        per_device, mesh=mesh, in_specs=placed, out_specs=P("ep", None, None), check_vma=False
    )
```

```python
import functools

import jax
import jax.numpy as jnp
from jax import lax
from jax.experimental import pallas as pl
from jax.experimental.pallas import tpu as pltpu
from jax.sharding import PartitionSpec as P

EPS = 1e-06
SLOTS = 8
LABELS = 128
FLAG_LANE = 64

f32 = jnp.float32
bf16 = jnp.bfloat16
i32 = jnp.int32


def iota(shape, dim):
    return lax.broadcasted_iota(i32, shape, dim)


def dot(a, b):
    return jnp.dot(a, b, preferred_element_type=f32)


def one_hot(mask):
    return jnp.where(mask, 1.0, 0.0).astype(bf16)


def spread(columns, top):
    rows = columns.shape[0]
    return jnp.concatenate(
        [jnp.broadcast_to(columns[:, k : k + 1], (rows, 128)) for k in range(top)], axis=0
    )


def dispatch_kernel(len_ref, tok, rt, gt, gain_ref, send_ref, aux_ref, normed_ref, x_s, r_s, g_s, *, base):
    seqs, new, features = tok.shape
    rows = seqs * new
    top = rt.shape[2]
    pairs = rows * top
    slots_all = send_ref.shape[0]
    for i in range(seqs):
        x_s[i * new : (i + 1) * new, :] = tok[i].astype(f32)
        r_s[i * new : (i + 1) * new, :] = rt[i]
        g_s[i * new : (i + 1) * new, :] = gt[i]

    wide = x_s[...]
    normed = wide * lax.rsqrt(jnp.mean(wide * wide, axis=-1, keepdims=True) + EPS) * gain_ref[...]
    normed = normed.astype(bf16)
    normed_ref[...] = normed

    token = iota((rows, 128), 0)
    length = jnp.zeros((rows, 128), i32)
    for s in range(seqs):
        length = jnp.where(token // new == s, len_ref[s], length)
    live = jnp.concatenate([jnp.where(token % new < length, 1, 0)] * top, axis=0) > 0
    expert = spread(r_s[...], top)
    gate = spread(g_s[...], top)

    chip = jnp.where(live, expert >> 2, -1).astype(f32)
    local = (expert & 3).astype(f32)
    i0, i1 = iota((pairs, pairs), 0), iota((pairs, pairs), 1)
    chip_row = jnp.sum(jnp.where(i0 == i1, chip, 0.0), axis=0, keepdims=True)
    equal = chip == chip_row
    pos_row = jnp.sum(jnp.where(equal & (i0 < i1), 1.0, 0.0), axis=0, keepdims=True).astype(i32)
    pos_col = jnp.sum(jnp.where(equal & (i1 < i0), 1.0, 0.0), axis=1, keepdims=True).astype(i32)

    def placed(where_to, pos):
        chip_i = where_to.astype(i32)
        slot = pos - base
        mine = (chip_i >= 0) & (slot >= 0) & (slot < SLOTS)
        return jnp.where(mine, chip_i * SLOTS + slot, -1)

    target_row = placed(chip_row, pos_row)
    target_col = placed(chip, jnp.broadcast_to(pos_col, chip.shape))
    over = jnp.where((chip_row >= 0.0) & (pos_row >= base + SLOTS), 1.0, 0.0)
    over = jnp.sum(over, axis=1, keepdims=True)

    lane = iota((pairs, LABELS), 1)
    labels = jnp.where(lane == 0, local + 1.0, 0.0).astype(bf16)
    aux_ref[...] = jnp.where(lane == 0, target_col.astype(f32), jnp.where(lane == 1, gate, 0.0))
    copies = jnp.concatenate([normed] * top, axis=0)
    step = 256
    flag_lane = iota((step, LABELS), 1) == FLAG_LANE
    for at in range(0, slots_all, step):
        picks = one_hot(iota((step, pairs), 0) + at == target_row)
        send_ref[at : at + step, :features] = dot(picks, copies).astype(bf16)
        marks = jnp.where(flag_lane, over, dot(picks, labels))
        send_ref[at : at + step, features:] = marks.astype(bf16)


def expert_kernel(
    core_ref, arrived_ref, gate_own, gate_sib, up_own, up_sib, down_own, down_sib,
    reply_ref, flag_ref, x_s, o_s,
):
    core = core_ref[0]
    own = gate_own.shape[0]
    features = reply_ref.shape[1]
    slots_all = arrived_ref.shape[0]

    r8, l8 = iota((8, LABELS), 0), iota((8, LABELS), 1)
    wanted = one_hot(((r8 == 0) & (l8 == 0)) | ((r8 == 1) & (l8 == FLAG_LANE)))
    found = lax.dot_general(
        wanted, arrived_ref[:, features:], (((1,), (1,)), ((), ())), preferred_element_type=f32
    )
    flag_ref[0] = jnp.where(jnp.sum(found[1:2]) > 0.0, 1, 0)
    ids = found[0:1].astype(i32)
    which = jnp.where(ids > 0, (ids - 1 + own * core) & (2 * own - 1), -1)
    hot = one_hot(iota((8, slots_all), 0) == which)
    earlier = one_hot(iota((slots_all, slots_all), 0) < iota((slots_all, slots_all), 1))
    rank = dot(hot, earlier).astype(i32)
    place = jnp.full((1, slots_all), -1, i32)
    start = jnp.int32(0)
    spans = []
    for j in range(2 * own):
        count = jnp.sum(jnp.where(which == j, 1.0, 0.0)).astype(i32)
        place = jnp.where(which == j, rank[j : j + 1] + start, place)
        spans.append((start, count))
        start = start + ((count + 15) // 16) * 16
    total = start

    blocks = (total + 127) // 128

    def gather(b, carry):
        at = pl.multiple_of(b * 128, 128)
        picks = one_hot(iota((128, slots_all), 0) + at == place)
        x_s[pl.ds(at, 128), :] = dot(picks, arrived_ref[:, :features]).astype(bf16)
        return carry

    lax.fori_loop(0, blocks, gather, 0)
    x_s[pl.ds(pl.multiple_of(blocks * 128, 128), 128), :] = jnp.zeros((128, features), bf16)
    o_s[:256, :] = jnp.zeros((256, features), bf16)

    @pl.when(total > 256)
    def _():
        o_s[256:512, :] = jnp.zeros((256, features), bf16)

    for j, (begin, count) in enumerate(spans):
        wg, wu, wd = (gate_own, up_own, down_own) if j < own else (gate_sib, up_sib, down_sib)

        def block(at, size, j=j % own, wg=wg, wu=wu, wd=wd):
            at = pl.multiple_of(at, 16)
            x = x_s[pl.ds(at, size), :]
            gate_part = dot(x, wg[j])
            up_part = dot(x, wu[j])
            hidden = (gate_part / (1.0 + jnp.exp(-gate_part)) * up_part).astype(bf16)
            o_s[pl.ds(at, size), :] = dot(hidden, wd[j]).astype(bf16)

        @pl.when((count > 0) & (count <= 64))
        def _(begin=begin, block=block):
            block(begin, 64)

        @pl.when(count > 64)
        def _(begin=begin, count=count, block=block):
            def body(b, carry):
                block(begin + b * 128, 128)
                return carry

            lax.fori_loop(0, (count + 127) // 128, body, 0)

    place_f = place.astype(f32)

    def scatter(depth):
        for at in range(0, slots_all, 256):
            same = iota((256, slots_all), 0) + at == iota((256, slots_all), 1)
            column = jnp.sum(jnp.where(same, place_f, 0.0), axis=1, keepdims=True).astype(i32)
            picks = one_hot(iota((256, depth), 1) == column)
            reply_ref[at : at + 256, :] = dot(picks, o_s[:depth, :]).astype(bf16)

    @pl.when(total <= 256)
    def _():
        scatter(256)

    @pl.when(total > 256)
    def _():
        scatter(512)


def fetched_sum(returned_ref, aux_ref, rows):
    pairs = aux_ref.shape[0]
    target = aux_ref[:, 0:1].astype(i32)
    picks = one_hot(iota((pairs, returned_ref.shape[0]), 1) == target)
    weighted = dot(picks, returned_ref[...]) * aux_ref[:, 1:2]
    total = weighted[:rows]
    for k in range(rows, pairs, rows):
        total = total + weighted[k : k + rows]
    return total


def combine_kernel(returned_ref, aux_ref, out_ref):
    out_ref[...] = fetched_sum(returned_ref, aux_ref, out_ref.shape[0])


def shared_kernel(normed_ref, gate_ref, up_ref, down_ref, out_ref):
    normed = normed_ref[...]
    gate_part = dot(normed, gate_ref[...])
    up_part = dot(normed, up_ref[...])
    hidden = (gate_part / (1.0 + jnp.exp(-gate_part)) * up_part).astype(bf16)
    out_ref[...] = dot(hidden, down_ref[...])


def final_kernel(len_ref, returned_ref, aux_ref, extra_ref, shared_ref, gain_ref, out_ref):
    seqs, new, features = out_ref.shape
    routed = fetched_sum(returned_ref, aux_ref, seqs * new) + extra_ref[...]
    summed = routed + shared_ref[...]
    mixed = summed * lax.rsqrt(jnp.mean(summed * summed, axis=-1, keepdims=True) + EPS) * gain_ref[...]
    for s in range(seqs):
        live = iota((new, features), 0) < len_ref[s]
        out_ref[s] = jnp.where(live, mixed[s * new : (s + 1) * new], 0.0).astype(bf16)


VMEM = pl.BlockSpec(memory_space=pltpu.VMEM)
SMEM = pl.BlockSpec(memory_space=pltpu.SMEM)


def limit(mib):
    return pltpu.CompilerParams(vmem_limit_bytes=mib * 1024 * 1024)


def per_device(
    tokens, lengths, routes, gates, norm_gain, expert_gate, expert_up, expert_down,
    shared_gate, shared_up, shared_down, out_gain,
):
    seqs, new, features = tokens.shape
    rows = seqs * new
    top = routes.shape[2]
    devices = lax.axis_size("ep")
    chips = devices // 2
    slots_all = chips * SLOTS
    pairs = rows * top
    core = (lax.axis_index("ep") & 1).astype(i32).reshape(1)
    groups = [[2 * c + k for c in range(chips)] for k in range(2)]
    sibling = functools.partial(lax.ppermute, axis_name="ep", perm=[(d, d ^ 1) for d in range(devices)])

    def dispatch(base):
        return pl.pallas_call(
            functools.partial(dispatch_kernel, base=base),
            out_shape=(
                jax.ShapeDtypeStruct((slots_all, features + LABELS), bf16),
                jax.ShapeDtypeStruct((pairs, 128), f32),
                jax.ShapeDtypeStruct((rows, features), bf16),
            ),
            in_specs=[SMEM] + [VMEM] * 4,
            out_specs=(VMEM, VMEM, VMEM),
            scratch_shapes=[
                pltpu.VMEM((rows, features), f32),
                pltpu.VMEM((rows, top), i32),
                pltpu.VMEM((rows, top), f32),
            ],
            compiler_params=limit(12),
            name="dispatch",
        )(lengths, tokens, routes, gates, norm_gain.reshape(1, features))

    def exchange(values):
        width = values.shape[1]
        return lax.all_to_all(
            values.reshape(chips, SLOTS, width), "ep", split_axis=0, concat_axis=0,
            axis_index_groups=groups, tiled=True,
        ).reshape(slots_all, width)

    def experts(arrived, weights):
        return pl.pallas_call(
            expert_kernel,
            out_shape=(
                jax.ShapeDtypeStruct((slots_all, features), bf16),
                jax.ShapeDtypeStruct((1,), i32),
            ),
            in_specs=[SMEM] + [VMEM] * 7,
            out_specs=(VMEM, SMEM),
            scratch_shapes=[
                pltpu.VMEM((slots_all + 128, features), bf16),
                pltpu.VMEM((slots_all + 128, features), bf16),
            ],
            compiler_params=limit(24),
            name="experts",
        )(core, arrived, *weights)

    send, aux, normed = dispatch(0)
    own = (expert_gate, expert_up, expert_down)
    weights = [w for v in own for w in (v, sibling(v))]

    arrived = exchange(send)
    replies, flag = experts(arrived, weights)
    shared = pl.pallas_call(
        shared_kernel,
        out_shape=jax.ShapeDtypeStruct((rows, features), f32),
        in_specs=[VMEM] * 4,
        out_specs=VMEM,
        compiler_params=limit(8),
        name="shared",
    )(normed, shared_gate, shared_up, shared_down)
    flags = flag + sibling(flag)
    returned = exchange(replies)
    flags, returned = lax.optimization_barrier((flags, returned))

    def second_round():
        send, aux, _ = dispatch(SLOTS)
        replies, _ = experts(exchange(send), weights)
        return pl.pallas_call(
            combine_kernel,
            out_shape=jax.ShapeDtypeStruct((rows, features), f32),
            in_specs=[VMEM] * 2,
            out_specs=VMEM,
            compiler_params=limit(8),
            name="combine",
        )(exchange(replies), aux)

    extra = lax.cond(flags[0] > 0, second_round, lambda: jnp.zeros((rows, features), f32))
    return pl.pallas_call(
        final_kernel,
        out_shape=jax.ShapeDtypeStruct(tokens.shape, bf16),
        in_specs=[SMEM] + [VMEM] * 5,
        out_specs=VMEM,
        compiler_params=limit(8),
        name="final",
    )(lengths, returned, aux, extra, shared, out_gain.reshape(1, features))


def solution(mesh):
    placed = (
        P("ep", None, None),
        P("ep"),
        P("ep", None, None),
        P("ep", None, None),
        P(),
        P("ep", None, None),
        P("ep", None, None),
        P("ep", None, None),
        P(),
        P(),
        P(),
        P(),
    )
    return jax.shard_map(
        per_device, mesh=mesh, in_specs=placed, out_specs=P("ep", None, None), check_vma=False
    )
```

```python
import functools

import jax
import jax.numpy as jnp
from jax import lax
from jax.experimental import pallas as pl
from jax.experimental.pallas import tpu as pltpu
from jax.sharding import PartitionSpec as P

EPS = 1e-06
SLOTS = 8
LABELS = 128
CHUNKS = 4
FLAG_LANE = 64

f32 = jnp.float32
bf16 = jnp.bfloat16
i32 = jnp.int32


def iota(shape, dim):
    return lax.broadcasted_iota(i32, shape, dim)


def dot(a, b):
    return jnp.dot(a, b, preferred_element_type=f32)


def one_hot(mask):
    return jnp.where(mask, 1.0, 0.0).astype(bf16)


def spread(columns, top):
    rows = columns.shape[0]
    return jnp.concatenate(
        [jnp.broadcast_to(columns[:, k : k + 1], (rows, 128)) for k in range(top)], axis=0
    )


def dispatch_kernel(len_ref, tok, rt, gt, gain_ref, send_hbm, aux_ref, normed_ref, x_s, r_s, g_s, send_s, sems, *, base):
    seqs, new, features = tok.shape
    rows = seqs * new
    top = rt.shape[2]
    pairs = rows * top
    slots_all = send_hbm.shape[0]
    for i in range(seqs):
        x_s[i * new : (i + 1) * new, :] = tok[i].astype(f32)
        r_s[i * new : (i + 1) * new, :] = rt[i]
        g_s[i * new : (i + 1) * new, :] = gt[i]

    wide = x_s[...]
    normed = wide * lax.rsqrt(jnp.mean(wide * wide, axis=-1, keepdims=True) + EPS) * gain_ref[...]
    normed = normed.astype(bf16)
    normed_ref[...] = normed

    token = iota((rows, 128), 0)
    length = jnp.zeros((rows, 128), i32)
    for s in range(seqs):
        length = jnp.where(token // new == s, len_ref[s], length)
    live = jnp.concatenate([jnp.where(token % new < length, 1, 0)] * top, axis=0) > 0
    expert = spread(r_s[...], top)
    gate = spread(g_s[...], top)

    chip = jnp.where(live, expert >> 2, -1).astype(f32)
    local = (expert & 3).astype(f32)
    i0, i1 = iota((pairs, pairs), 0), iota((pairs, pairs), 1)
    chip_row = jnp.sum(jnp.where(i0 == i1, chip, 0.0), axis=0, keepdims=True)
    equal = chip == chip_row
    pos_row = jnp.sum(jnp.where(equal & (i0 < i1), 1.0, 0.0), axis=0, keepdims=True).astype(i32)
    pos_col = jnp.sum(jnp.where(equal & (i1 < i0), 1.0, 0.0), axis=1, keepdims=True).astype(i32)

    def placed(where_to, pos):
        chip_i = where_to.astype(i32)
        slot = pos - base
        mine = (chip_i >= 0) & (slot >= 0) & (slot < SLOTS)
        return jnp.where(mine, chip_i * SLOTS + slot, -1)

    target_row = placed(chip_row, pos_row)
    target_col = placed(chip, jnp.broadcast_to(pos_col, chip.shape))
    over = jnp.where((chip_row >= 0.0) & (pos_row >= base + SLOTS), 1.0, 0.0)
    over = jnp.sum(over, axis=1, keepdims=True)

    lane = iota((pairs, LABELS), 1)
    labels = jnp.where(lane == 0, local + 1.0, 0.0).astype(bf16)
    aux_ref[...] = jnp.where(lane == 0, target_col.astype(f32), jnp.where(lane == 1, gate, 0.0))
    copies = jnp.concatenate([normed] * top, axis=0)
    step = slots_all // CHUNKS
    flag_lane = iota((step, LABELS), 1) == FLAG_LANE
    outward = []
    for c in range(CHUNKS):
        at = c * step
        picks = one_hot(iota((step, pairs), 0) + at == target_row)
        send_s[at : at + step, :features] = dot(picks, copies).astype(bf16)
        marks = jnp.where(flag_lane, over, dot(picks, labels))
        send_s[at : at + step, features:] = marks.astype(bf16)
        part = pl.ds(at, step)
        outward.append(pltpu.make_async_copy(send_s.at[part], send_hbm.at[part], sems.at[c]))
        outward[-1].start()
    for copy in outward:
        copy.wait()


def expert_kernel(
    core_ref, arrived_ref, gate_hbm, gate_sib, up_hbm, up_sib, down_hbm, down_sib_hbm,
    reply_hbm, flag_ref, x_s, o_s, reply_s, gate_own, up_own, down_own, down_sib, sems, weight_sems,
):
    core = core_ref[0]
    own = gate_own.shape[0]
    inward = [
        pltpu.make_async_copy(source, target, weight_sems.at[i])
        for i, (source, target) in enumerate(
            ((down_sib_hbm, down_sib), (gate_hbm, gate_own), (up_hbm, up_own), (down_hbm, down_own))
        )
    ]
    for copy in inward:
        copy.start()
    features = reply_hbm.shape[1]
    slots_all = arrived_ref.shape[0]

    r8, l8 = iota((8, LABELS), 0), iota((8, LABELS), 1)
    wanted = one_hot(((r8 == 0) & (l8 == 0)) | ((r8 == 1) & (l8 == FLAG_LANE)))
    found = lax.dot_general(
        wanted, arrived_ref[:, features:], (((1,), (1,)), ((), ())), preferred_element_type=f32
    )
    flag_ref[0] = jnp.where(jnp.sum(found[1:2]) > 0.0, 1, 0)
    ids = found[0:1].astype(i32)
    which = jnp.where(ids > 0, (ids - 1 + own * core + own) & (2 * own - 1), -1)
    hot = one_hot(iota((8, slots_all), 0) == which)
    earlier = one_hot(iota((slots_all, slots_all), 0) < iota((slots_all, slots_all), 1))
    rank = dot(hot, earlier).astype(i32)
    place = jnp.full((1, slots_all), -1, i32)
    start = jnp.int32(0)
    spans = []
    for j in range(2 * own):
        count = jnp.sum(jnp.where(which == j, 1.0, 0.0)).astype(i32)
        place = jnp.where(which == j, rank[j : j + 1] + start, place)
        spans.append((start, count))
        start = start + ((count + 15) // 16) * 16
    total = start
    most = slots_all + 128

    blocks = (total + 127) // 128

    def gather(b, carry):
        at = pl.multiple_of(b * 128, 128)
        picks = one_hot(iota((128, slots_all), 0) + at == place)
        x_s[pl.ds(at, 128), :] = dot(picks, arrived_ref[:, :features]).astype(bf16)
        return carry

    lax.fori_loop(0, blocks, gather, 0)
    x_s[pl.ds(pl.multiple_of(blocks * 128, 128), 128), :] = jnp.zeros((128, features), bf16)
    o_s[:256, :] = jnp.zeros((256, features), bf16)

    @pl.when(total > 256)
    def _():
        o_s[256:most, :] = jnp.zeros((most - 256, features), bf16)

    for j, (begin, count) in enumerate(spans):
        wg, wu, wd = (gate_sib, up_sib, down_sib) if j < own else (gate_own, up_own, down_own)
        if j == 0:
            inward[0].wait()
        if j == own:
            for copy in inward[1:]:
                copy.wait()

        def block(at, size, j=j % own, wg=wg, wu=wu, wd=wd):
            at = pl.multiple_of(at, 16)
            x = x_s[pl.ds(at, size), :]
            gate_part = dot(x, wg[j])
            up_part = dot(x, wu[j])
            hidden = (gate_part / (1.0 + jnp.exp(-gate_part)) * up_part).astype(bf16)
            o_s[pl.ds(at, size), :] = dot(hidden, wd[j]).astype(bf16)

        @pl.when((count > 0) & (count <= 64))
        def _(begin=begin, block=block):
            block(begin, 64)

        @pl.when(count > 64)
        def _(begin=begin, count=count, block=block):
            def body(b, carry):
                block(begin + b * 128, 128)
                return carry

            lax.fori_loop(0, (count + 127) // 128, body, 0)

    place_f = place.astype(f32)

    def scatter(depth):
        step = slots_all // CHUNKS
        outward = []
        for c in range(CHUNKS):
            at = c * step
            same = iota((step, slots_all), 0) + at == iota((step, slots_all), 1)
            column = jnp.sum(jnp.where(same, place_f, 0.0), axis=1, keepdims=True).astype(i32)
            picks = one_hot(iota((step, depth), 1) == column)
            reply_s[at : at + step, :] = dot(picks, o_s[:depth, :]).astype(bf16)
            part = pl.ds(at, step)
            outward.append(pltpu.make_async_copy(reply_s.at[part], reply_hbm.at[part], sems.at[c]))
            outward[-1].start()
        for copy in outward:
            copy.wait()

    @pl.when(total <= 256)
    def _():
        scatter(256)

    @pl.when(total > 256)
    def _():
        scatter(most)


def fetched_sum(returned_ref, aux_ref, rows):
    pairs = aux_ref.shape[0]
    target = aux_ref[:, 0:1].astype(i32)
    picks = one_hot(iota((pairs, returned_ref.shape[0]), 1) == target)
    weighted = dot(picks, returned_ref[...]) * aux_ref[:, 1:2]
    total = weighted[:rows]
    for k in range(rows, pairs, rows):
        total = total + weighted[k : k + rows]
    return total


def combine_kernel(returned_ref, aux_ref, out_ref):
    out_ref[...] = fetched_sum(returned_ref, aux_ref, out_ref.shape[0])


def shared_kernel(normed_ref, gate_ref, up_ref, down_ref, gain_ref, out_ref, gain_out):
    normed = normed_ref[...]
    gate_part = dot(normed, gate_ref[...])
    up_part = dot(normed, up_ref[...])
    hidden = (gate_part / (1.0 + jnp.exp(-gate_part)) * up_part).astype(bf16)
    out_ref[...] = dot(hidden, down_ref[...])
    gain_out[...] = gain_ref[...]


def final_kernel(len_ref, returned_ref, aux_ref, extra_ref, shared_ref, gain_ref, out_ref):
    seqs, new, features = out_ref.shape
    routed = fetched_sum(returned_ref, aux_ref, seqs * new) + extra_ref[...]
    summed = routed + shared_ref[...]
    mixed = summed * lax.rsqrt(jnp.mean(summed * summed, axis=-1, keepdims=True) + EPS) * gain_ref[...]
    for s in range(seqs):
        live = iota((new, features), 0) < len_ref[s]
        out_ref[s] = jnp.where(live, mixed[s * new : (s + 1) * new], 0.0).astype(bf16)


VMEM = pl.BlockSpec(memory_space=pltpu.VMEM)
SMEM = pl.BlockSpec(memory_space=pltpu.SMEM)
HBM = pl.BlockSpec(memory_space=pltpu.HBM)


def limit(mib):
    return pltpu.CompilerParams(vmem_limit_bytes=mib * 1024 * 1024)


def per_device(
    tokens, lengths, routes, gates, norm_gain, expert_gate, expert_up, expert_down,
    shared_gate, shared_up, shared_down, out_gain,
):
    seqs, new, features = tokens.shape
    rows = seqs * new
    top = routes.shape[2]
    devices = lax.axis_size("ep")
    chips = devices // 2
    slots_all = chips * SLOTS
    pairs = rows * top
    core = (lax.axis_index("ep") & 1).astype(i32).reshape(1)
    groups = [[2 * c + k for c in range(chips)] for k in range(2)]
    sibling = functools.partial(lax.ppermute, axis_name="ep", perm=[(d, d ^ 1) for d in range(devices)])

    def dispatch(base):
        return pl.pallas_call(
            functools.partial(dispatch_kernel, base=base),
            out_shape=(
                jax.ShapeDtypeStruct((slots_all, features + LABELS), bf16),
                jax.ShapeDtypeStruct((pairs, 128), f32),
                jax.ShapeDtypeStruct((rows, features), bf16),
            ),
            in_specs=[SMEM] + [VMEM] * 4,
            out_specs=(HBM, VMEM, VMEM),
            scratch_shapes=[
                pltpu.VMEM((rows, features), f32),
                pltpu.VMEM((rows, top), i32),
                pltpu.VMEM((rows, top), f32),
                pltpu.VMEM((slots_all, features + LABELS), bf16),
                pltpu.SemaphoreType.DMA((CHUNKS,)),
            ],
            compiler_params=limit(12),
            name="dispatch",
        )(lengths, tokens, routes, gates, norm_gain.reshape(1, features))

    def exchange(values):
        width = values.shape[1]
        return lax.all_to_all(
            values.reshape(chips, SLOTS, width), "ep", split_axis=0, concat_axis=0,
            axis_index_groups=groups, tiled=True,
        ).reshape(slots_all, width)

    def experts(arrived, weights):
        return pl.pallas_call(
            expert_kernel,
            out_shape=(
                jax.ShapeDtypeStruct((slots_all, features), bf16),
                jax.ShapeDtypeStruct((1,), i32),
            ),
            in_specs=[SMEM, VMEM, HBM, VMEM, HBM, VMEM, HBM, HBM],
            out_specs=(HBM, SMEM),
            scratch_shapes=[
                pltpu.VMEM((slots_all + 256, features), bf16),
                pltpu.VMEM((slots_all + 256, features), bf16),
                pltpu.VMEM((slots_all, features), bf16),
                *[pltpu.VMEM(w.shape, bf16) for w in (*own, expert_down)],
                pltpu.SemaphoreType.DMA((CHUNKS,)),
                pltpu.SemaphoreType.DMA((4,)),
            ],
            compiler_params=limit(24),
            name="experts",
        )(core, arrived, *weights)

    own = (expert_gate, expert_up, expert_down)
    send, aux, normed = dispatch(0)
    weights = [w for v in own for w in (v, sibling(v))]

    arrived = exchange(send)
    replies, flag = experts(arrived, weights)
    shared, gain = pl.pallas_call(
        shared_kernel,
        out_shape=(
            jax.ShapeDtypeStruct((rows, features), f32),
            jax.ShapeDtypeStruct((1, features), f32),
        ),
        in_specs=[VMEM] * 5,
        out_specs=(VMEM, VMEM),
        compiler_params=limit(8),
        name="shared",
    )(normed, shared_gate, shared_up, shared_down, out_gain.reshape(1, features))
    flags = flag + sibling(flag)
    returned = exchange(replies)
    flags, returned = lax.optimization_barrier((flags, returned))

    def second_round():
        send, aux, _ = dispatch(SLOTS)
        again = lax.optimization_barrier((send, *own))
        weights = [w for v in again[1:] for w in (v, sibling(v))]
        replies, _ = experts(exchange(again[0]), weights)
        return pl.pallas_call(
            combine_kernel,
            out_shape=jax.ShapeDtypeStruct((rows, features), f32),
            in_specs=[VMEM] * 2,
            out_specs=VMEM,
            compiler_params=limit(8),
            name="combine",
        )(exchange(replies), aux)

    extra = lax.cond(flags[0] > 0, second_round, lambda: jnp.zeros((rows, features), f32))
    return pl.pallas_call(
        final_kernel,
        out_shape=jax.ShapeDtypeStruct(tokens.shape, bf16),
        in_specs=[SMEM] + [VMEM] * 5,
        out_specs=VMEM,
        compiler_params=limit(8),
        name="final",
    )(lengths, returned, aux, extra, shared, gain)


def solution(mesh):
    placed = (
        P("ep", None, None),
        P("ep"),
        P("ep", None, None),
        P("ep", None, None),
        P(),
        P("ep", None, None),
        P("ep", None, None),
        P("ep", None, None),
        P(),
        P(),
        P(),
        P(),
    )
    return jax.shard_map(
        per_device, mesh=mesh, in_specs=placed, out_specs=P("ep", None, None), check_vma=False
    )
```

```python
import functools

import jax
import jax.numpy as jnp
from jax import lax
from jax.experimental import pallas as pl
from jax.experimental.pallas import tpu as pltpu
from jax.sharding import PartitionSpec as P

EPS = 1e-06
SLOTS = 8
LABELS = 128
CHUNKS = 4
FLAG_LANE = 64

f32 = jnp.float32
bf16 = jnp.bfloat16
i32 = jnp.int32


def iota(shape, dim):
    return lax.broadcasted_iota(i32, shape, dim)


def dot(a, b):
    return jnp.dot(a, b, preferred_element_type=f32)


def one_hot(mask):
    return jnp.where(mask, 1.0, 0.0).astype(bf16)


def spread(columns, top):
    rows = columns.shape[0]
    return jnp.concatenate(
        [jnp.broadcast_to(columns[:, k : k + 1], (rows, 128)) for k in range(top)], axis=0
    )


def dispatch_kernel(len_ref, tok, rt, gt, gain_ref, send_hbm, aux_ref, normed_ref, x_s, r_s, g_s, send_s, sems, *, base):
    seqs, new, features = tok.shape
    rows = seqs * new
    top = rt.shape[2]
    pairs = rows * top
    slots_all = send_hbm.shape[0]
    for i in range(seqs):
        x_s[i * new : (i + 1) * new, :] = tok[i].astype(f32)
        r_s[i * new : (i + 1) * new, :] = rt[i]
        g_s[i * new : (i + 1) * new, :] = gt[i]

    wide = x_s[...]
    normed = wide * lax.rsqrt(jnp.mean(wide * wide, axis=-1, keepdims=True) + EPS) * gain_ref[...]
    normed = normed.astype(bf16)
    normed_ref[...] = normed

    token = iota((rows, 128), 0)
    length = jnp.zeros((rows, 128), i32)
    for s in range(seqs):
        length = jnp.where(token // new == s, len_ref[s], length)
    live = jnp.concatenate([jnp.where(token % new < length, 1, 0)] * top, axis=0) > 0
    expert = spread(r_s[...], top)
    gate = spread(g_s[...], top)

    chip = jnp.where(live, expert >> 2, -1).astype(f32)
    local = (expert & 3).astype(f32)
    i0, i1 = iota((pairs, pairs), 0), iota((pairs, pairs), 1)
    chip_row = jnp.sum(jnp.where(i0 == i1, chip, 0.0), axis=0, keepdims=True)
    equal = chip == chip_row
    pos_row = jnp.sum(jnp.where(equal & (i0 < i1), 1.0, 0.0), axis=0, keepdims=True).astype(i32)
    pos_col = jnp.sum(jnp.where(equal & (i1 < i0), 1.0, 0.0), axis=1, keepdims=True).astype(i32)

    def placed(where_to, pos):
        chip_i = where_to.astype(i32)
        slot = pos - base
        mine = (chip_i >= 0) & (slot >= 0) & (slot < SLOTS)
        return jnp.where(mine, chip_i * SLOTS + slot, -1)

    target_row = placed(chip_row, pos_row)
    target_col = placed(chip, jnp.broadcast_to(pos_col, chip.shape))
    over = jnp.where((chip_row >= 0.0) & (pos_row >= base + SLOTS), 1.0, 0.0)
    over = jnp.sum(over, axis=1, keepdims=True)

    lane = iota((pairs, LABELS), 1)
    labels = jnp.where(lane == 0, local + 1.0, 0.0).astype(bf16)
    alive = jnp.where(live, 1.0, 0.0)
    aux_ref[...] = jnp.where(
        lane == 0, target_col.astype(f32), jnp.where(lane == 1, gate, jnp.where(lane == 2, alive, 0.0))
    )
    copies = jnp.concatenate([normed] * top, axis=0)
    step = slots_all // CHUNKS
    flag_lane = iota((step, LABELS), 1) == FLAG_LANE
    outward = []
    for c in range(CHUNKS):
        at = c * step
        picks = one_hot(iota((step, pairs), 0) + at == target_row)
        send_s[at : at + step, :features] = dot(picks, copies).astype(bf16)
        marks = jnp.where(flag_lane, over, dot(picks, labels))
        send_s[at : at + step, features:] = marks.astype(bf16)
        part = pl.ds(at, step)
        outward.append(pltpu.make_async_copy(send_s.at[part], send_hbm.at[part], sems.at[c]))
        outward[-1].start()
    for copy in outward:
        copy.wait()


def expert_kernel(
    core_ref, arrived_ref, gate_hbm, gate_sib, up_hbm, up_sib, down_hbm, down_sib_hbm,
    reply_hbm, flag_ref, x_s, o_s, reply_s, gate_own, up_own, down_own, down_sib, sems, weight_sems,
):
    core = jnp.concatenate([core_ref[0:1, :]] * (arrived_ref.shape[0] // 128), axis=1)
    own = gate_own.shape[0]
    inward = [
        pltpu.make_async_copy(source, target, weight_sems.at[i])
        for i, (source, target) in enumerate(
            ((down_sib_hbm, down_sib), (gate_hbm, gate_own), (up_hbm, up_own), (down_hbm, down_own))
        )
    ]
    for copy in inward:
        copy.start()
    features = reply_hbm.shape[1]
    slots_all = arrived_ref.shape[0]

    r8, l8 = iota((8, LABELS), 0), iota((8, LABELS), 1)
    wanted = one_hot(((r8 == 0) & (l8 == 0)) | ((r8 == 1) & (l8 == FLAG_LANE)))
    found = lax.dot_general(
        wanted, arrived_ref[:, features:], (((1,), (1,)), ((), ())), preferred_element_type=f32
    )
    flag_ref[0] = jnp.where(jnp.sum(found[1:2]) > 0.0, 1, 0)
    ids = found[0:1].astype(i32)
    which = jnp.where(ids > 0, (ids - 1 + own * core + own) & (2 * own - 1), -1)
    hot = one_hot(iota((8, slots_all), 0) == which)
    earlier = one_hot(iota((slots_all, slots_all), 0) < iota((slots_all, slots_all), 1))
    rank = dot(hot, earlier).astype(i32)
    place = jnp.full((1, slots_all), -1, i32)
    start = jnp.int32(0)
    spans = []
    for j in range(2 * own):
        count = jnp.sum(jnp.where(which == j, 1.0, 0.0)).astype(i32)
        place = jnp.where(which == j, rank[j : j + 1] + start, place)
        spans.append((start, count))
        start = start + ((count + 15) // 16) * 16
    total = start
    most = slots_all + 128

    blocks = (total + 127) // 128

    def gather(b, carry):
        at = pl.multiple_of(b * 128, 128)
        picks = one_hot(iota((128, slots_all), 0) + at == place)
        x_s[pl.ds(at, 128), :] = dot(picks, arrived_ref[:, :features]).astype(bf16)
        return carry

    lax.fori_loop(0, blocks, gather, 0)
    x_s[pl.ds(pl.multiple_of(blocks * 128, 128), 128), :] = jnp.zeros((128, features), bf16)
    o_s[:256, :] = jnp.zeros((256, features), bf16)

    @pl.when(total > 256)
    def _():
        o_s[256:most, :] = jnp.zeros((most - 256, features), bf16)

    for j, (begin, count) in enumerate(spans):
        wg, wu, wd = (gate_sib, up_sib, down_sib) if j < own else (gate_own, up_own, down_own)
        if j == 0:
            inward[0].wait()
        if j == own:
            for copy in inward[1:]:
                copy.wait()

        def block(at, size, j=j % own, wg=wg, wu=wu, wd=wd):
            at = pl.multiple_of(at, 16)
            x = x_s[pl.ds(at, size), :]
            gate_part = dot(x, wg[j])
            up_part = dot(x, wu[j])
            hidden = (gate_part / (1.0 + jnp.exp(-gate_part)) * up_part).astype(bf16)
            o_s[pl.ds(at, size), :] = dot(hidden, wd[j]).astype(bf16)

        @pl.when((count > 0) & (count <= 64))
        def _(begin=begin, block=block):
            block(begin, 64)

        @pl.when(count > 64)
        def _(begin=begin, count=count, block=block):
            def body(b, carry):
                block(begin + b * 128, 128)
                return carry

            lax.fori_loop(0, (count + 127) // 128, body, 0)

    place_f = place.astype(f32)

    def scatter(depth):
        step = slots_all // CHUNKS
        outward = []
        for c in range(CHUNKS):
            at = c * step
            same = iota((step, slots_all), 0) + at == iota((step, slots_all), 1)
            column = jnp.sum(jnp.where(same, place_f, 0.0), axis=1, keepdims=True).astype(i32)
            picks = one_hot(iota((step, depth), 1) == column)
            reply_s[at : at + step, :] = dot(picks, o_s[:depth, :]).astype(bf16)
            part = pl.ds(at, step)
            outward.append(pltpu.make_async_copy(reply_s.at[part], reply_hbm.at[part], sems.at[c]))
            outward[-1].start()
        for copy in outward:
            copy.wait()

    @pl.when(total <= 256)
    def _():
        scatter(256)

    @pl.when(total > 256)
    def _():
        scatter(most)


def fetched_sum(returned_ref, aux_ref, rows):
    pairs = aux_ref.shape[0]
    target = aux_ref[:, 0:1].astype(i32)
    picks = one_hot(iota((pairs, returned_ref.shape[0]), 1) == target)
    weighted = dot(picks, returned_ref[...]) * aux_ref[:, 1:2]
    total = weighted[:rows]
    for k in range(rows, pairs, rows):
        total = total + weighted[k : k + rows]
    return total


def combine_kernel(returned_ref, aux_ref, out_ref):
    out_ref[...] = fetched_sum(returned_ref, aux_ref, out_ref.shape[0])


def shared_kernel(normed_ref, gate_ref, up_ref, down_ref, gain_ref, out_ref, gain_out):
    normed = normed_ref[...]
    gate_part = dot(normed, gate_ref[...])
    up_part = dot(normed, up_ref[...])
    hidden = (gate_part / (1.0 + jnp.exp(-gate_part)) * up_part).astype(bf16)
    out_ref[...] = dot(hidden, down_ref[...])
    gain_out[...] = gain_ref[...]


def final_kernel(returned_ref, aux_ref, extra_ref, shared_ref, gain_ref, out_ref):
    seqs, new, features = out_ref.shape
    routed = fetched_sum(returned_ref, aux_ref, seqs * new) + extra_ref[...]
    summed = routed + shared_ref[...]
    mixed = summed * lax.rsqrt(jnp.mean(summed * summed, axis=-1, keepdims=True) + EPS) * gain_ref[...]
    mixed = jnp.where(aux_ref[: seqs * new, 2:3] > 0.0, mixed, 0.0)
    for s in range(seqs):
        out_ref[s] = mixed[s * new : (s + 1) * new].astype(bf16)


VMEM = pl.BlockSpec(memory_space=pltpu.VMEM)
SMEM = pl.BlockSpec(memory_space=pltpu.SMEM)
HBM = pl.BlockSpec(memory_space=pltpu.HBM)


def limit(mib):
    return pltpu.CompilerParams(vmem_limit_bytes=mib * 1024 * 1024)


def per_device(
    tokens, lengths, routes, gates, norm_gain, expert_gate, expert_up, expert_down,
    shared_gate, shared_up, shared_down, out_gain,
):
    seqs, new, features = tokens.shape
    rows = seqs * new
    top = routes.shape[2]
    devices = lax.axis_size("ep")
    chips = devices // 2
    slots_all = chips * SLOTS
    pairs = rows * top
    core = jnp.full((8, 128), (lax.axis_index("ep") & 1).astype(i32))
    groups = [[2 * c + k for c in range(chips)] for k in range(2)]
    sibling = functools.partial(lax.ppermute, axis_name="ep", perm=[(d, d ^ 1) for d in range(devices)])

    def dispatch(base):
        return pl.pallas_call(
            functools.partial(dispatch_kernel, base=base),
            out_shape=(
                jax.ShapeDtypeStruct((slots_all, features + LABELS), bf16),
                jax.ShapeDtypeStruct((pairs, 128), f32),
                jax.ShapeDtypeStruct((rows, features), bf16),
            ),
            in_specs=[SMEM] + [VMEM] * 4,
            out_specs=(HBM, VMEM, VMEM),
            scratch_shapes=[
                pltpu.VMEM((rows, features), f32),
                pltpu.VMEM((rows, top), i32),
                pltpu.VMEM((rows, top), f32),
                pltpu.VMEM((slots_all, features + LABELS), bf16),
                pltpu.SemaphoreType.DMA((CHUNKS,)),
            ],
            compiler_params=limit(12),
            name="dispatch",
        )(lengths, tokens, routes, gates, norm_gain.reshape(1, features))

    def exchange(values):
        width = values.shape[1]
        return lax.all_to_all(
            values.reshape(chips, SLOTS, width), "ep", split_axis=0, concat_axis=0,
            axis_index_groups=groups, tiled=True,
        ).reshape(slots_all, width)

    def experts(arrived, weights):
        return pl.pallas_call(
            expert_kernel,
            out_shape=(
                jax.ShapeDtypeStruct((slots_all, features), bf16),
                jax.ShapeDtypeStruct((1,), i32),
            ),
            in_specs=[VMEM, VMEM, HBM, VMEM, HBM, VMEM, HBM, HBM],
            out_specs=(HBM, SMEM),
            scratch_shapes=[
                pltpu.VMEM((slots_all + 256, features), bf16),
                pltpu.VMEM((slots_all + 256, features), bf16),
                pltpu.VMEM((slots_all, features), bf16),
                *[pltpu.VMEM(w.shape, bf16) for w in (*own, expert_down)],
                pltpu.SemaphoreType.DMA((CHUNKS,)),
                pltpu.SemaphoreType.DMA((4,)),
            ],
            compiler_params=limit(24),
            name="experts",
        )(core, arrived, *weights)

    own = (expert_gate, expert_up, expert_down)
    send, aux, normed = dispatch(0)
    weights = [w for v in own for w in (v, sibling(v))]

    arrived = exchange(send)
    replies, flag = experts(arrived, weights)
    shared, gain = pl.pallas_call(
        shared_kernel,
        out_shape=(
            jax.ShapeDtypeStruct((rows, features), f32),
            jax.ShapeDtypeStruct((1, features), f32),
        ),
        in_specs=[VMEM] * 5,
        out_specs=(VMEM, VMEM),
        compiler_params=limit(8),
        name="shared",
    )(normed, shared_gate, shared_up, shared_down, out_gain.reshape(1, features))
    flags = flag + sibling(flag)
    returned = exchange(replies)
    flags, returned = lax.optimization_barrier((flags, returned))

    def second_round():
        send, aux, _ = dispatch(SLOTS)
        again = lax.optimization_barrier((send, *own))
        weights = [w for v in again[1:] for w in (v, sibling(v))]
        replies, _ = experts(exchange(again[0]), weights)
        return pl.pallas_call(
            combine_kernel,
            out_shape=jax.ShapeDtypeStruct((rows, features), f32),
            in_specs=[VMEM] * 2,
            out_specs=VMEM,
            compiler_params=limit(8),
            name="combine",
        )(exchange(replies), aux)

    extra = lax.cond(flags[0] > 0, second_round, lambda: jnp.zeros((rows, features), f32))
    return pl.pallas_call(
        final_kernel,
        out_shape=jax.ShapeDtypeStruct(tokens.shape, bf16),
        in_specs=[VMEM] * 5,
        out_specs=VMEM,
        compiler_params=limit(8),
        name="final",
    )(returned, aux, extra, shared, gain)


def solution(mesh):
    placed = (
        P("ep", None, None),
        P("ep"),
        P("ep", None, None),
        P("ep", None, None),
        P(),
        P("ep", None, None),
        P("ep", None, None),
        P("ep", None, None),
        P(),
        P(),
        P(),
        P(),
    )
    return jax.shard_map(
        per_device, mesh=mesh, in_specs=placed, out_specs=P("ep", None, None), check_vma=False
    )
```

```python
import functools

import jax
import jax.numpy as jnp
from jax import lax
from jax.experimental import pallas as pl
from jax.experimental.pallas import tpu as pltpu
from jax.sharding import PartitionSpec as P

EPS = 1e-06
SLOTS = 8
LABELS = 128
CHUNKS = 4
FLAG_LANE = 64

f32 = jnp.float32
bf16 = jnp.bfloat16
i32 = jnp.int32


def iota(shape, dim):
    return lax.broadcasted_iota(i32, shape, dim)


def dot(a, b):
    return jnp.dot(a, b, preferred_element_type=f32)


def one_hot(mask):
    return jnp.where(mask, 1.0, 0.0).astype(bf16)


def spread(columns, top):
    rows = columns.shape[0]
    return jnp.concatenate(
        [jnp.broadcast_to(columns[:, k : k + 1], (rows, 128)) for k in range(top)], axis=0
    )


def dispatch_kernel(len_ref, tok, rt, gt, gain_ref, send_hbm, aux_ref, normed_ref, x_s, r_s, g_s, send_s, sems, *, base):
    seqs, new, features = tok.shape
    rows = seqs * new
    top = rt.shape[2]
    pairs = rows * top
    slots_all = send_hbm.shape[0]
    for i in range(seqs):
        x_s[i * new : (i + 1) * new, :] = tok[i].astype(f32)
        r_s[i * new : (i + 1) * new, :] = rt[i]
        g_s[i * new : (i + 1) * new, :] = gt[i]

    wide = x_s[...]
    normed = wide * lax.rsqrt(jnp.mean(wide * wide, axis=-1, keepdims=True) + EPS) * gain_ref[...]
    normed = normed.astype(bf16)
    normed_ref[...] = normed

    token = iota((rows, 128), 0)
    length = jnp.zeros((rows, 128), i32)
    for s in range(seqs):
        length = jnp.where(token // new == s, len_ref[s], length)
    live = jnp.concatenate([jnp.where(token % new < length, 1, 0)] * top, axis=0) > 0
    expert = spread(r_s[...], top)
    gate = spread(g_s[...], top)

    chip = jnp.where(live, expert >> 2, -1).astype(f32)
    local = (expert & 3).astype(f32)
    i0, i1 = iota((pairs, pairs), 0), iota((pairs, pairs), 1)
    chip_row = jnp.sum(jnp.where(i0 == i1, chip, 0.0), axis=0, keepdims=True)
    equal = chip == chip_row
    pos_row = jnp.sum(jnp.where(equal & (i0 < i1), 1.0, 0.0), axis=0, keepdims=True).astype(i32)
    pos_col = jnp.sum(jnp.where(equal & (i1 < i0), 1.0, 0.0), axis=1, keepdims=True).astype(i32)

    def placed(where_to, pos):
        chip_i = where_to.astype(i32)
        slot = pos - base
        mine = (chip_i >= 0) & (slot >= 0) & (slot < SLOTS)
        return jnp.where(mine, chip_i * SLOTS + slot, -1)

    target_row = placed(chip_row, pos_row)
    target_col = placed(chip, jnp.broadcast_to(pos_col, chip.shape))
    over = jnp.where((chip_row >= 0.0) & (pos_row >= base + SLOTS), 1.0, 0.0)
    over = jnp.sum(over, axis=1, keepdims=True)

    lane = iota((pairs, LABELS), 1)
    labels = jnp.where(lane == 0, local + 1.0, 0.0).astype(bf16)
    alive = jnp.where(live, 1.0, 0.0)
    aux_ref[...] = jnp.where(
        lane == 0, target_col.astype(f32), jnp.where(lane == 1, gate, jnp.where(lane == 2, alive, 0.0))
    )
    copies = jnp.concatenate([normed] * top, axis=0)
    step = slots_all // CHUNKS
    flag_lane = iota((step, LABELS), 1) == FLAG_LANE
    outward = []
    for c in range(CHUNKS):
        at = c * step
        picks = one_hot(iota((step, pairs), 0) + at == target_row)
        send_s[at : at + step, :features] = dot(picks, copies).astype(bf16)
        marks = jnp.where(flag_lane, over, dot(picks, labels))
        send_s[at : at + step, features:] = marks.astype(bf16)
        part = pl.ds(at, step)
        outward.append(pltpu.make_async_copy(send_s.at[part], send_hbm.at[part], sems.at[c]))
        outward[-1].start()
    for copy in outward:
        copy.wait()


def expert_kernel(
    core_ref, arrived_ref, gate_hbm, gate_sib, up_hbm, up_sib, down_hbm, down_sib_hbm,
    reply_hbm, flag_ref, x_s, o_s, reply_s, gate_own, up_own, down_own, down_sib, sems, weight_sems,
):
    core = jnp.concatenate([core_ref[0:1, :]] * (arrived_ref.shape[0] // 128), axis=1)
    own = gate_own.shape[0]
    inward = [
        pltpu.make_async_copy(source, target, weight_sems.at[i])
        for i, (source, target) in enumerate(
            ((down_sib_hbm, down_sib), (gate_hbm, gate_own), (up_hbm, up_own), (down_hbm, down_own))
        )
    ]
    for copy in inward:
        copy.start()
    features = reply_hbm.shape[1]
    slots_all = arrived_ref.shape[0]

    r8, l8 = iota((8, LABELS), 0), iota((8, LABELS), 1)
    wanted = one_hot(((r8 == 0) & (l8 == 0)) | ((r8 == 1) & (l8 == FLAG_LANE)))
    found = lax.dot_general(
        wanted, arrived_ref[:, features:], (((1,), (1,)), ((), ())), preferred_element_type=f32
    )
    flag_ref[0] = jnp.where(jnp.sum(found[1:2]) > 0.0, 1, 0)
    ids = found[0:1].astype(i32)
    which = jnp.where(ids > 0, (ids - 1 + own * core + own) & (2 * own - 1), -1)
    hot = one_hot(iota((8, slots_all), 0) == which)
    earlier = one_hot(iota((slots_all, slots_all), 0) < iota((slots_all, slots_all), 1))
    rank = dot(hot, earlier).astype(i32)
    place = jnp.full((1, slots_all), -1, i32)
    start = jnp.int32(0)
    spans = []
    for j in range(2 * own):
        count = jnp.sum(jnp.where(which == j, 1.0, 0.0)).astype(i32)
        place = jnp.where(which == j, rank[j : j + 1] + start, place)
        spans.append((start, count))
        start = start + ((count + 15) // 16) * 16
    total = start
    most = slots_all + 128

    blocks = (total + 127) // 128

    def gather(b, carry):
        at = pl.multiple_of(b * 128, 128)
        picks = one_hot(iota((128, slots_all), 0) + at == place)
        x_s[pl.ds(at, 128), :] = dot(picks, arrived_ref[:, :features]).astype(bf16)
        return carry

    lax.fori_loop(0, blocks, gather, 0)
    x_s[pl.ds(pl.multiple_of(blocks * 128, 128), 128), :] = jnp.zeros((128, features), bf16)
    o_s[:256, :] = jnp.zeros((256, features), bf16)

    @pl.when(total > 256)
    def _():
        o_s[256:most, :] = jnp.zeros((most - 256, features), bf16)

    for j, (begin, count) in enumerate(spans):
        wg, wu, wd = (gate_sib, up_sib, down_sib) if j < own else (gate_own, up_own, down_own)
        if j == 0:
            inward[0].wait()
        if j == own:
            for copy in inward[1:]:
                copy.wait()

        def block(at, size, j=j % own, wg=wg, wu=wu, wd=wd):
            at = pl.multiple_of(at, 16)
            x = x_s[pl.ds(at, size), :]
            gate_part = dot(x, wg[j])
            up_part = dot(x, wu[j])
            hidden = (gate_part / (1.0 + jnp.exp(-gate_part)) * up_part).astype(bf16)
            o_s[pl.ds(at, size), :] = dot(hidden, wd[j]).astype(bf16)

        @pl.when((count > 0) & (count <= 64))
        def _(begin=begin, block=block):
            block(begin, 64)

        @pl.when(count > 64)
        def _(begin=begin, count=count, block=block):
            def body(b, carry):
                block(begin + b * 128, 128)
                return carry

            lax.fori_loop(0, (count + 127) // 128, body, 0)

    place_f = place.astype(f32)

    def scatter(depth):
        step = slots_all // CHUNKS
        outward = []
        for c in range(CHUNKS):
            at = c * step
            same = iota((step, slots_all), 0) + at == iota((step, slots_all), 1)
            column = jnp.sum(jnp.where(same, place_f, 0.0), axis=1, keepdims=True).astype(i32)
            picks = one_hot(iota((step, depth), 1) == column)
            reply_s[at : at + step, :] = dot(picks, o_s[:depth, :]).astype(bf16)
            part = pl.ds(at, step)
            outward.append(pltpu.make_async_copy(reply_s.at[part], reply_hbm.at[part], sems.at[c]))
            outward[-1].start()
        for copy in outward:
            copy.wait()

    @pl.when(total <= 256)
    def _():
        scatter(256)

    @pl.when(total > 256)
    def _():
        scatter(most)


def fetched_sum(returned_ref, aux_ref, rows):
    pairs = aux_ref.shape[0]
    target = aux_ref[:, 0:1].astype(i32)
    picks = one_hot(iota((pairs, returned_ref.shape[0]), 1) == target)
    weighted = dot(picks, returned_ref[...]) * aux_ref[:, 1:2]
    total = weighted[:rows]
    for k in range(rows, pairs, rows):
        total = total + weighted[k : k + rows]
    return total


def combine_kernel(returned_ref, aux_ref, out_ref):
    out_ref[...] = fetched_sum(returned_ref, aux_ref, out_ref.shape[0])


def shared_kernel(normed_ref, gate_ref, up_ref, down_ref, gain_ref, out_ref, gain_out):
    normed = normed_ref[...]
    gate_part = dot(normed, gate_ref[...])
    up_part = dot(normed, up_ref[...])
    hidden = (gate_part / (1.0 + jnp.exp(-gate_part)) * up_part).astype(bf16)
    out_ref[...] = dot(hidden, down_ref[...])
    gain_out[...] = gain_ref[...]


def final_kernel(returned_ref, aux_ref, extra_ref, shared_ref, gain_ref, out_ref):
    seqs, new, features = out_ref.shape
    routed = fetched_sum(returned_ref, aux_ref, seqs * new) + extra_ref[...]
    summed = routed + shared_ref[...]
    mixed = summed * lax.rsqrt(jnp.mean(summed * summed, axis=-1, keepdims=True) + EPS) * gain_ref[...]
    mixed = jnp.where(aux_ref[: seqs * new, 2:3] > 0.0, mixed, 0.0)
    for s in range(seqs):
        out_ref[s] = mixed[s * new : (s + 1) * new].astype(bf16)


VMEM = pl.BlockSpec(memory_space=pltpu.VMEM)
SMEM = pl.BlockSpec(memory_space=pltpu.SMEM)
HBM = pl.BlockSpec(memory_space=pltpu.HBM)


def limit(mib):
    return pltpu.CompilerParams(vmem_limit_bytes=mib * 1024 * 1024)


def per_device(
    tokens, lengths, routes, gates, norm_gain, expert_gate, expert_up, expert_down,
    shared_gate, shared_up, shared_down, out_gain,
):
    seqs, new, features = tokens.shape
    rows = seqs * new
    top = routes.shape[2]
    devices = lax.axis_size("ep")
    chips = devices // 2
    slots_all = chips * SLOTS
    pairs = rows * top
    core = jnp.full((8, 128), (lax.axis_index("ep") & 1).astype(i32))
    groups = [[2 * c + k for c in range(chips)] for k in range(2)]
    sibling = functools.partial(lax.ppermute, axis_name="ep", perm=[(d, d ^ 1) for d in range(devices)])

    def dispatch(base):
        return pl.pallas_call(
            functools.partial(dispatch_kernel, base=base),
            out_shape=(
                pltpu.HBM((slots_all, features + LABELS), bf16),
                jax.ShapeDtypeStruct((pairs, 128), f32),
                jax.ShapeDtypeStruct((rows, features), bf16),
            ),
            in_specs=[SMEM] + [VMEM] * 4,
            out_specs=(HBM, VMEM, VMEM),
            scratch_shapes=[
                pltpu.VMEM((rows, features), f32),
                pltpu.VMEM((rows, top), i32),
                pltpu.VMEM((rows, top), f32),
                pltpu.VMEM((slots_all, features + LABELS), bf16),
                pltpu.SemaphoreType.DMA((CHUNKS,)),
            ],
            compiler_params=limit(12),
            name="dispatch",
        )(lengths, tokens, routes, gates, norm_gain.reshape(1, features))

    def exchange(values):
        width = values.shape[1]
        return lax.all_to_all(
            values.reshape(chips, SLOTS, width), "ep", split_axis=0, concat_axis=0,
            axis_index_groups=groups, tiled=True,
        ).reshape(slots_all, width)

    def experts(arrived, weights):
        return pl.pallas_call(
            expert_kernel,
            out_shape=(
                pltpu.HBM((slots_all, features), bf16),
                jax.ShapeDtypeStruct((1,), i32),
            ),
            in_specs=[VMEM, VMEM, HBM, VMEM, HBM, VMEM, HBM, HBM],
            out_specs=(HBM, SMEM),
            scratch_shapes=[
                pltpu.VMEM((slots_all + 256, features), bf16),
                pltpu.VMEM((slots_all + 256, features), bf16),
                pltpu.VMEM((slots_all, features), bf16),
                *[pltpu.VMEM(w.shape, bf16) for w in (*own, expert_down)],
                pltpu.SemaphoreType.DMA((CHUNKS,)),
                pltpu.SemaphoreType.DMA((4,)),
            ],
            compiler_params=limit(24),
            name="experts",
        )(core, arrived, *weights)

    own = (expert_gate, expert_up, expert_down)
    send, aux, normed = dispatch(0)
    weights = [w for v in own for w in (v, sibling(v))]

    arrived = exchange(send)
    replies, flag = experts(arrived, weights)
    shared, gain = pl.pallas_call(
        shared_kernel,
        out_shape=(
            jax.ShapeDtypeStruct((rows, features), f32),
            jax.ShapeDtypeStruct((1, features), f32),
        ),
        in_specs=[VMEM] * 5,
        out_specs=(VMEM, VMEM),
        compiler_params=limit(8),
        name="shared",
    )(normed, shared_gate, shared_up, shared_down, out_gain.reshape(1, features))
    flags = flag + sibling(flag)
    returned = exchange(replies)
    flags, returned = lax.optimization_barrier((flags, returned))

    def second_round():
        send, aux, _ = dispatch(SLOTS)
        again = lax.optimization_barrier((send, *own))
        weights = [w for v in again[1:] for w in (v, sibling(v))]
        replies, _ = experts(exchange(again[0]), weights)
        return pl.pallas_call(
            combine_kernel,
            out_shape=jax.ShapeDtypeStruct((rows, features), f32),
            in_specs=[VMEM] * 2,
            out_specs=VMEM,
            compiler_params=limit(8),
            name="combine",
        )(exchange(replies), aux)

    extra = lax.cond(flags[0] > 0, second_round, lambda: jnp.zeros((rows, features), f32))
    return pl.pallas_call(
        final_kernel,
        out_shape=jax.ShapeDtypeStruct(tokens.shape, bf16),
        in_specs=[VMEM] * 5,
        out_specs=VMEM,
        compiler_params=limit(8),
        name="final",
    )(returned, aux, extra, shared, gain)


def solution(mesh):
    placed = (
        P("ep", None, None),
        P("ep"),
        P("ep", None, None),
        P("ep", None, None),
        P(),
        P("ep", None, None),
        P("ep", None, None),
        P("ep", None, None),
        P(),
        P(),
        P(),
        P(),
    )
    return jax.shard_map(
        per_device, mesh=mesh, in_specs=placed, out_specs=P("ep", None, None), check_vma=False
    )
```

```python
import functools

import jax
import jax.numpy as jnp
from jax import lax
from jax.experimental import pallas as pl
from jax.experimental.pallas import tpu as pltpu
from jax.sharding import PartitionSpec as P

EPS = 1e-06
SLOTS = 8
LABELS = 128
CHUNKS = 4
FLAG_LANE = 64

f32 = jnp.float32
bf16 = jnp.bfloat16
i32 = jnp.int32


def iota(shape, dim):
    return lax.broadcasted_iota(i32, shape, dim)


def dot(a, b):
    return jnp.dot(a, b, preferred_element_type=f32)


def one_hot(mask):
    return jnp.where(mask, 1.0, 0.0).astype(bf16)


def spread(columns, top):
    rows = columns.shape[0]
    return jnp.concatenate(
        [jnp.broadcast_to(columns[:, k : k + 1], (rows, 128)) for k in range(top)], axis=0
    )


def dispatch_kernel(len_ref, tok, rt, gt, gain_ref, send_hbm, aux_ref, normed_ref, x_s, r_s, g_s, send_s, sems, *, base):
    seqs, new, features = tok.shape
    rows = seqs * new
    top = rt.shape[2]
    pairs = rows * top
    slots_all = send_hbm.shape[0]
    for i in range(seqs):
        x_s[i * new : (i + 1) * new, :] = tok[i].astype(f32)
        r_s[i * new : (i + 1) * new, :] = rt[i]
        g_s[i * new : (i + 1) * new, :] = gt[i]

    wide = x_s[...]
    normed = wide * lax.rsqrt(jnp.mean(wide * wide, axis=-1, keepdims=True) + EPS) * gain_ref[...]
    normed = normed.astype(bf16)
    normed_ref[...] = normed

    token = iota((rows, 128), 0)
    length = jnp.zeros((rows, 128), i32)
    for s in range(seqs):
        length = jnp.where(token // new == s, len_ref[s], length)
    live = jnp.concatenate([jnp.where(token % new < length, 1, 0)] * top, axis=0) > 0
    expert = spread(r_s[...], top)
    gate = spread(g_s[...], top)

    chip = jnp.where(live, expert >> 2, -1).astype(f32)
    local = (expert & 3).astype(f32)
    i0, i1 = iota((pairs, pairs), 0), iota((pairs, pairs), 1)
    chip_row = jnp.sum(jnp.where(i0 == i1, chip, 0.0), axis=0, keepdims=True)
    equal = chip == chip_row
    pos_row = jnp.sum(jnp.where(equal & (i0 < i1), 1.0, 0.0), axis=0, keepdims=True).astype(i32)
    pos_col = jnp.sum(jnp.where(equal & (i1 < i0), 1.0, 0.0), axis=1, keepdims=True).astype(i32)

    def placed(where_to, pos):
        chip_i = where_to.astype(i32)
        slot = pos - base
        mine = (chip_i >= 0) & (slot >= 0) & (slot < SLOTS)
        return jnp.where(mine, chip_i * SLOTS + slot, -1)

    target_row = placed(chip_row, pos_row)
    target_col = placed(chip, jnp.broadcast_to(pos_col, chip.shape))
    over = jnp.where((chip_row >= 0.0) & (pos_row >= base + SLOTS), 1.0, 0.0)
    over = jnp.sum(over, axis=1, keepdims=True)

    lane = iota((pairs, LABELS), 1)
    labels = jnp.where(lane == 0, local + 1.0, 0.0).astype(bf16)
    alive = jnp.where(live, 1.0, 0.0)
    aux_ref[...] = jnp.where(
        lane == 0, target_col.astype(f32), jnp.where(lane == 1, gate, jnp.where(lane == 2, alive, 0.0))
    )
    copies = jnp.concatenate([normed] * top, axis=0)
    step = slots_all // CHUNKS
    flag_lane = iota((step, LABELS), 1) == FLAG_LANE
    outward = []
    for c in range(CHUNKS):
        at = c * step
        picks = one_hot(iota((step, pairs), 0) + at == target_row)
        send_s[at : at + step, :features] = dot(picks, copies).astype(bf16)
        marks = jnp.where(flag_lane, over, dot(picks, labels))
        send_s[at : at + step, features:] = marks.astype(bf16)
        part = pl.ds(at, step)
        outward.append(pltpu.make_async_copy(send_s.at[part], send_hbm.at[part], sems.at[c]))
        outward[-1].start()
    for copy in outward:
        copy.wait()


def expert_kernel(
    core_ref, arrived_ref, gate_hbm, gate_sib, up_hbm, up_sib, down_hbm, down_sib_hbm,
    reply_hbm, flag_ref, x_s, o_s, reply_s, gate_own, up_own, down_own, down_sib, sems, weight_sems,
):
    core = jnp.concatenate([core_ref[0:1, :]] * (arrived_ref.shape[0] // 128), axis=1)
    own = gate_own.shape[0]
    parts = [(down_sib_hbm, down_sib)]
    for e in range(own):
        parts += [
            (gate_hbm.at[e], gate_own.at[e]), (up_hbm.at[e], up_own.at[e]), (down_hbm.at[e], down_own.at[e])
        ]
    inward = [
        pltpu.make_async_copy(source, target, weight_sems.at[i])
        for i, (source, target) in enumerate(parts)
    ]
    for copy in inward:
        copy.start()
    features = reply_hbm.shape[1]
    slots_all = arrived_ref.shape[0]

    r8, l8 = iota((8, LABELS), 0), iota((8, LABELS), 1)
    wanted = one_hot(((r8 == 0) & (l8 == 0)) | ((r8 == 1) & (l8 == FLAG_LANE)))
    found = lax.dot_general(
        wanted, arrived_ref[:, features:], (((1,), (1,)), ((), ())), preferred_element_type=f32
    )
    flag_ref[0] = jnp.where(jnp.sum(found[1:2]) > 0.0, 1, 0)
    ids = found[0:1].astype(i32)
    which = jnp.where(ids > 0, (ids - 1 + own * core + own) & (2 * own - 1), -1)
    hot = one_hot(iota((8, slots_all), 0) == which)
    earlier = one_hot(iota((slots_all, slots_all), 0) < iota((slots_all, slots_all), 1))
    rank = dot(hot, earlier).astype(i32)
    place = jnp.full((1, slots_all), -1, i32)
    start = jnp.int32(0)
    spans = []
    for j in range(2 * own):
        count = jnp.sum(jnp.where(which == j, 1.0, 0.0)).astype(i32)
        place = jnp.where(which == j, rank[j : j + 1] + start, place)
        spans.append((start, count))
        start = start + ((count + 15) // 16) * 16
    total = start
    most = slots_all + 128

    blocks = (total + 127) // 128

    def gather(b, carry):
        at = pl.multiple_of(b * 128, 128)
        picks = one_hot(iota((128, slots_all), 0) + at == place)
        x_s[pl.ds(at, 128), :] = dot(picks, arrived_ref[:, :features]).astype(bf16)
        return carry

    lax.fori_loop(0, blocks, gather, 0)
    x_s[pl.ds(pl.multiple_of(blocks * 128, 128), 128), :] = jnp.zeros((128, features), bf16)
    o_s[:256, :] = jnp.zeros((256, features), bf16)

    @pl.when(total > 256)
    def _():
        o_s[256:most, :] = jnp.zeros((most - 256, features), bf16)

    for j, (begin, count) in enumerate(spans):
        wg, wu, wd = (gate_sib, up_sib, down_sib) if j < own else (gate_own, up_own, down_own)
        if j == 0:
            inward[0].wait()
        if j >= own:
            for copy in inward[1 + 3 * (j - own) : 4 + 3 * (j - own)]:
                copy.wait()

        def block(at, size, j=j % own, wg=wg, wu=wu, wd=wd):
            at = pl.multiple_of(at, 16)
            x = x_s[pl.ds(at, size), :]
            gate_part = dot(x, wg[j])
            up_part = dot(x, wu[j])
            hidden = (gate_part / (1.0 + jnp.exp(-gate_part)) * up_part).astype(bf16)
            o_s[pl.ds(at, size), :] = dot(hidden, wd[j]).astype(bf16)

        @pl.when((count > 0) & (count <= 64))
        def _(begin=begin, block=block):
            block(begin, 64)

        @pl.when(count > 64)
        def _(begin=begin, count=count, block=block):
            def body(b, carry):
                block(begin + b * 128, 128)
                return carry

            lax.fori_loop(0, (count + 127) // 128, body, 0)

    place_f = place.astype(f32)

    def scatter(depth):
        step = slots_all // CHUNKS
        outward = []
        for c in range(CHUNKS):
            at = c * step
            same = iota((step, slots_all), 0) + at == iota((step, slots_all), 1)
            column = jnp.sum(jnp.where(same, place_f, 0.0), axis=1, keepdims=True).astype(i32)
            picks = one_hot(iota((step, depth), 1) == column)
            reply_s[at : at + step, :] = dot(picks, o_s[:depth, :]).astype(bf16)
            part = pl.ds(at, step)
            outward.append(pltpu.make_async_copy(reply_s.at[part], reply_hbm.at[part], sems.at[c]))
            outward[-1].start()
        for copy in outward:
            copy.wait()

    @pl.when(total <= 256)
    def _():
        scatter(256)

    @pl.when(total > 256)
    def _():
        scatter(most)


def fetched_sum(returned_ref, aux_ref, rows):
    pairs = aux_ref.shape[0]
    target = aux_ref[:, 0:1].astype(i32)
    picks = one_hot(iota((pairs, returned_ref.shape[0]), 1) == target)
    weighted = dot(picks, returned_ref[...]) * aux_ref[:, 1:2]
    total = weighted[:rows]
    for k in range(rows, pairs, rows):
        total = total + weighted[k : k + rows]
    return total


def combine_kernel(returned_ref, aux_ref, out_ref):
    out_ref[...] = fetched_sum(returned_ref, aux_ref, out_ref.shape[0])


def shared_kernel(normed_ref, gate_ref, up_ref, down_ref, gain_ref, out_ref, gain_out):
    normed = normed_ref[...]
    gate_part = dot(normed, gate_ref[...])
    up_part = dot(normed, up_ref[...])
    hidden = (gate_part / (1.0 + jnp.exp(-gate_part)) * up_part).astype(bf16)
    out_ref[...] = dot(hidden, down_ref[...])
    gain_out[...] = gain_ref[...]


def final_kernel(returned_ref, aux_ref, extra_ref, shared_ref, gain_ref, out_ref):
    seqs, new, features = out_ref.shape
    routed = fetched_sum(returned_ref, aux_ref, seqs * new) + extra_ref[...]
    summed = routed + shared_ref[...]
    mixed = summed * lax.rsqrt(jnp.mean(summed * summed, axis=-1, keepdims=True) + EPS) * gain_ref[...]
    mixed = jnp.where(aux_ref[: seqs * new, 2:3] > 0.0, mixed, 0.0)
    for s in range(seqs):
        out_ref[s] = mixed[s * new : (s + 1) * new].astype(bf16)


VMEM = pl.BlockSpec(memory_space=pltpu.VMEM)
SMEM = pl.BlockSpec(memory_space=pltpu.SMEM)
HBM = pl.BlockSpec(memory_space=pltpu.HBM)


def limit(mib):
    return pltpu.CompilerParams(vmem_limit_bytes=mib * 1024 * 1024)


def per_device(
    tokens, lengths, routes, gates, norm_gain, expert_gate, expert_up, expert_down,
    shared_gate, shared_up, shared_down, out_gain,
):
    seqs, new, features = tokens.shape
    rows = seqs * new
    top = routes.shape[2]
    devices = lax.axis_size("ep")
    chips = devices // 2
    slots_all = chips * SLOTS
    pairs = rows * top
    core = jnp.full((8, 128), (lax.axis_index("ep") & 1).astype(i32))
    groups = [[2 * c + k for c in range(chips)] for k in range(2)]
    sibling = functools.partial(lax.ppermute, axis_name="ep", perm=[(d, d ^ 1) for d in range(devices)])

    def dispatch(base):
        return pl.pallas_call(
            functools.partial(dispatch_kernel, base=base),
            out_shape=(
                pltpu.HBM((slots_all, features + LABELS), bf16),
                jax.ShapeDtypeStruct((pairs, 128), f32),
                jax.ShapeDtypeStruct((rows, features), bf16),
            ),
            in_specs=[SMEM] + [VMEM] * 4,
            out_specs=(HBM, VMEM, VMEM),
            scratch_shapes=[
                pltpu.VMEM((rows, features), f32),
                pltpu.VMEM((rows, top), i32),
                pltpu.VMEM((rows, top), f32),
                pltpu.VMEM((slots_all, features + LABELS), bf16),
                pltpu.SemaphoreType.DMA((CHUNKS,)),
            ],
            compiler_params=limit(12),
            name="dispatch",
        )(lengths, tokens, routes, gates, norm_gain.reshape(1, features))

    def exchange(values):
        width = values.shape[1]
        return lax.all_to_all(
            values.reshape(chips, SLOTS, width), "ep", split_axis=0, concat_axis=0,
            axis_index_groups=groups, tiled=True,
        ).reshape(slots_all, width)

    def experts(arrived, weights):
        return pl.pallas_call(
            expert_kernel,
            out_shape=(
                pltpu.HBM((slots_all, features), bf16),
                jax.ShapeDtypeStruct((1,), i32),
            ),
            in_specs=[VMEM, VMEM, HBM, VMEM, HBM, VMEM, HBM, HBM],
            out_specs=(HBM, SMEM),
            scratch_shapes=[
                pltpu.VMEM((slots_all + 256, features), bf16),
                pltpu.VMEM((slots_all + 256, features), bf16),
                pltpu.VMEM((slots_all, features), bf16),
                *[pltpu.VMEM(w.shape, bf16) for w in (*own, expert_down)],
                pltpu.SemaphoreType.DMA((CHUNKS,)),
                pltpu.SemaphoreType.DMA((1 + 3 * expert_gate.shape[0],)),
            ],
            compiler_params=limit(24),
            name="experts",
        )(core, arrived, *weights)

    own = (expert_gate, expert_up, expert_down)
    send, aux, normed = dispatch(0)
    weights = [w for v in own for w in (v, sibling(v))]

    arrived = exchange(send)
    replies, flag = experts(arrived, weights)
    shared, gain = pl.pallas_call(
        shared_kernel,
        out_shape=(
            jax.ShapeDtypeStruct((rows, features), f32),
            jax.ShapeDtypeStruct((1, features), f32),
        ),
        in_specs=[VMEM] * 5,
        out_specs=(VMEM, VMEM),
        compiler_params=limit(8),
        name="shared",
    )(normed, shared_gate, shared_up, shared_down, out_gain.reshape(1, features))
    flags = flag + sibling(flag)
    returned = exchange(replies)
    flags, returned = lax.optimization_barrier((flags, returned))

    def second_round():
        send, aux, _ = dispatch(SLOTS)
        again = lax.optimization_barrier((send, *own))
        weights = [w for v in again[1:] for w in (v, sibling(v))]
        replies, _ = experts(exchange(again[0]), weights)
        return pl.pallas_call(
            combine_kernel,
            out_shape=jax.ShapeDtypeStruct((rows, features), f32),
            in_specs=[VMEM] * 2,
            out_specs=VMEM,
            compiler_params=limit(8),
            name="combine",
        )(exchange(replies), aux)

    extra = lax.cond(flags[0] > 0, second_round, lambda: jnp.zeros((rows, features), f32))
    return pl.pallas_call(
        final_kernel,
        out_shape=jax.ShapeDtypeStruct(tokens.shape, bf16),
        in_specs=[VMEM] * 5,
        out_specs=VMEM,
        compiler_params=limit(8),
        name="final",
    )(returned, aux, extra, shared, gain)


def solution(mesh):
    placed = (
        P("ep", None, None),
        P("ep"),
        P("ep", None, None),
        P("ep", None, None),
        P(),
        P("ep", None, None),
        P("ep", None, None),
        P("ep", None, None),
        P(),
        P(),
        P(),
        P(),
    )
    return jax.shard_map(
        per_device, mesh=mesh, in_specs=placed, out_specs=P("ep", None, None), check_vma=False
    )
```

```python
import functools

import jax
import jax.numpy as jnp
from jax import lax
from jax.experimental import pallas as pl
from jax.experimental.pallas import tpu as pltpu
from jax.sharding import PartitionSpec as P

EPS = 1e-06
SLOTS = 8
LABELS = 128
CHUNKS = 4
FLAG_LANE = 64

f32 = jnp.float32
bf16 = jnp.bfloat16
i32 = jnp.int32


def iota(shape, dim):
    return lax.broadcasted_iota(i32, shape, dim)


def dot(a, b):
    return jnp.dot(a, b, preferred_element_type=f32)


def one_hot(mask):
    return jnp.where(mask, 1.0, 0.0).astype(bf16)


def spread(columns, top):
    rows = columns.shape[0]
    return jnp.concatenate(
        [jnp.broadcast_to(columns[:, k : k + 1], (rows, 128)) for k in range(top)], axis=0
    )


def dispatch_kernel(len_ref, tok, rt, gt, gain_ref, send_hbm, aux_ref, normed_ref, x_s, r_s, g_s, send_s, sems, *, base):
    seqs, new, features = tok.shape
    rows = seqs * new
    top = rt.shape[2]
    pairs = rows * top
    slots_all = send_hbm.shape[0]
    for i in range(seqs):
        x_s[i * new : (i + 1) * new, :] = tok[i].astype(f32)
        r_s[i * new : (i + 1) * new, :] = rt[i]
        g_s[i * new : (i + 1) * new, :] = gt[i]

    wide = x_s[...]
    normed = wide * lax.rsqrt(jnp.mean(wide * wide, axis=-1, keepdims=True) + EPS) * gain_ref[...]
    normed = normed.astype(bf16)
    normed_ref[...] = normed

    token = iota((rows, 128), 0)
    length = jnp.zeros((rows, 128), i32)
    for s in range(seqs):
        length = jnp.where(token // new == s, len_ref[s], length)
    live = jnp.concatenate([jnp.where(token % new < length, 1, 0)] * top, axis=0) > 0
    expert = spread(r_s[...], top)
    gate = spread(g_s[...], top)

    chip = jnp.where(live, expert >> 2, -1).astype(f32)
    local = (expert & 3).astype(f32)
    i0, i1 = iota((pairs, pairs), 0), iota((pairs, pairs), 1)
    chip_row = jnp.sum(jnp.where(i0 == i1, chip, 0.0), axis=0, keepdims=True)
    equal = chip == chip_row
    pos_row = jnp.sum(jnp.where(equal & (i0 < i1), 1.0, 0.0), axis=0, keepdims=True).astype(i32)
    pos_col = jnp.sum(jnp.where(equal & (i1 < i0), 1.0, 0.0), axis=1, keepdims=True).astype(i32)

    def placed(where_to, pos):
        chip_i = where_to.astype(i32)
        slot = pos - base
        mine = (chip_i >= 0) & (slot >= 0) & (slot < SLOTS)
        return jnp.where(mine, chip_i * SLOTS + slot, -1)

    target_row = placed(chip_row, pos_row)
    target_col = placed(chip, jnp.broadcast_to(pos_col, chip.shape))
    over = jnp.where((chip_row >= 0.0) & (pos_row >= base + SLOTS), 1.0, 0.0)
    over = jnp.sum(over, axis=1, keepdims=True)

    lane = iota((pairs, LABELS), 1)
    labels = jnp.where(lane == 0, local + 1.0, 0.0).astype(bf16)
    alive = jnp.where(live, 1.0, 0.0)
    aux_ref[...] = jnp.where(
        lane == 0, target_col.astype(f32), jnp.where(lane == 1, gate, jnp.where(lane == 2, alive, 0.0))
    )
    copies = jnp.concatenate([normed] * top, axis=0)
    step = slots_all // CHUNKS
    flag_lane = iota((step, LABELS), 1) == FLAG_LANE
    outward = []
    for c in range(CHUNKS):
        at = c * step
        picks = one_hot(iota((step, pairs), 0) + at == target_row)
        send_s[at : at + step, :features] = dot(picks, copies).astype(bf16)
        marks = jnp.where(flag_lane, over, dot(picks, labels))
        send_s[at : at + step, features:] = marks.astype(bf16)
        part = pl.ds(at, step)
        outward.append(pltpu.make_async_copy(send_s.at[part], send_hbm.at[part], sems.at[c]))
        outward[-1].start()
    for copy in outward:
        copy.wait()


def expert_kernel(
    core_ref, arrived_ref, gate_hbm, gate_sib, up_hbm, up_sib, down_hbm, down_sib_hbm,
    reply_hbm, flag_ref, x_s, o_s, reply_s, gate_own, up_own, down_own, down_sib, sems, weight_sems,
):
    core = jnp.concatenate([core_ref[0:1, :]] * (arrived_ref.shape[0] // 128), axis=1)
    own = gate_own.shape[0]
    parts = [(down_sib_hbm, down_sib)]
    for e in range(own):
        parts += [
            (gate_hbm.at[e], gate_own.at[e]), (up_hbm.at[e], up_own.at[e]), (down_hbm.at[e], down_own.at[e])
        ]
    inward = [
        pltpu.make_async_copy(source, target, weight_sems.at[i])
        for i, (source, target) in enumerate(parts)
    ]
    for copy in inward:
        copy.start()
    features = reply_hbm.shape[1]
    slots_all = arrived_ref.shape[0]

    r8, l8 = iota((8, LABELS), 0), iota((8, LABELS), 1)
    wanted = one_hot(((r8 == 0) & (l8 == 0)) | ((r8 == 1) & (l8 == FLAG_LANE)))
    found = lax.dot_general(
        wanted, arrived_ref[:, features:], (((1,), (1,)), ((), ())), preferred_element_type=f32
    )
    flag_ref[0] = jnp.where(jnp.sum(found[1:2]) > 0.0, 1, 0)
    ids = found[0:1].astype(i32)
    which = jnp.where(ids > 0, (ids - 1 + own * core + own) & (2 * own - 1), -1)
    hot = one_hot(iota((8, slots_all), 0) == which)
    earlier = one_hot(iota((slots_all, slots_all), 0) < iota((slots_all, slots_all), 1))
    rank = dot(hot, earlier).astype(i32)
    place = jnp.full((1, slots_all), -1, i32)
    start = jnp.int32(0)
    spans = []
    for j in range(2 * own):
        count = jnp.sum(jnp.where(which == j, 1.0, 0.0)).astype(i32)
        place = jnp.where(which == j, rank[j : j + 1] + start, place)
        spans.append((start, count))
        start = start + ((count + 15) // 16) * 16
    total = start
    most = slots_all + 128

    blocks = (total + 127) // 128

    def gather(b, carry):
        at = pl.multiple_of(b * 128, 128)
        picks = one_hot(iota((128, slots_all), 0) + at == place)
        x_s[pl.ds(at, 128), :] = dot(picks, arrived_ref[:, :features]).astype(bf16)
        return carry

    lax.fori_loop(0, blocks, gather, 0)
    x_s[pl.ds(pl.multiple_of(blocks * 128, 128), 128), :] = jnp.zeros((128, features), bf16)
    o_s[:256, :] = jnp.zeros((256, features), bf16)

    @pl.when(total > 256)
    def _():
        o_s[256:most, :] = jnp.zeros((most - 256, features), bf16)

    def run(items, size):
        rows = [x_s[pl.ds(pl.multiple_of(at, 16), size), :] for at, _, _ in items]
        gates = [dot(x, w[0][e]) for x, (_, w, e) in zip(rows, items)]
        ups = [dot(x, w[1][e]) for x, (_, w, e) in zip(rows, items)]
        mids = [(g / (1.0 + jnp.exp(-g)) * u).astype(bf16) for g, u in zip(gates, ups)]
        outs = [dot(h, w[2][e]).astype(bf16) for h, (_, w, e) in zip(mids, items)]
        for out, (at, _, _) in zip(outs, items):
            o_s[pl.ds(pl.multiple_of(at, 16), size), :] = out

    def chosen(e, values):
        picked = values[0]
        for k, value in enumerate(values[1:], 1):
            picked = jnp.where(e == k, value, picked)
        return picked

    for lowest, w in ((0, (gate_sib, up_sib, down_sib)), (own, (gate_own, up_own, down_own))):
        for copy in inward[:1] if lowest == 0 else inward[1:]:
            copy.wait()
        group = spans[lowest : lowest + own]

        def expert(e, carry, group=group, w=w):
            begin = chosen(e, [g[0] for g in group])
            count = chosen(e, [g[1] for g in group])

            @pl.when((count > 0) & (count <= 64))
            def _():
                run([(begin, w, e)], 64)

            @pl.when(count > 64)
            def _():
                def body(b, carry):
                    run([(begin + b * 128, w, e)], 128)
                    return carry

                lax.fori_loop(0, (count + 127) // 128, body, 0)

            return carry

        lax.fori_loop(0, own, expert, 0)

    place_f = place.astype(f32)
    step = slots_all // CHUNKS

    def outward(c):
        part = pl.ds(pl.multiple_of(c * step, step), step)
        return pltpu.make_async_copy(reply_s.at[part], reply_hbm.at[part], sems.at[c])

    def scatter(depth):
        def chunk(c, carry):
            at = pl.multiple_of(c * step, step)
            same = iota((step, slots_all), 0) + at == iota((step, slots_all), 1)
            column = jnp.sum(jnp.where(same, place_f, 0.0), axis=1, keepdims=True).astype(i32)
            picks = one_hot(iota((step, depth), 1) == column)
            reply_s[pl.ds(at, step), :] = dot(picks, o_s[:depth, :]).astype(bf16)
            outward(c).start()
            return carry

        lax.fori_loop(0, CHUNKS, chunk, 0)

    @pl.when(total <= 256)
    def _():
        scatter(256)

    @pl.when(total > 256)
    def _():
        scatter(most)

    for c in range(CHUNKS):
        outward(c).wait()


def fetched_sum(returned_ref, aux_ref, rows):
    pairs = aux_ref.shape[0]
    target = aux_ref[:, 0:1].astype(i32)
    picks = one_hot(iota((pairs, returned_ref.shape[0]), 1) == target)
    weighted = dot(picks, returned_ref[...]) * aux_ref[:, 1:2]
    total = weighted[:rows]
    for k in range(rows, pairs, rows):
        total = total + weighted[k : k + rows]
    return total


def combine_kernel(returned_ref, aux_ref, out_ref):
    out_ref[...] = fetched_sum(returned_ref, aux_ref, out_ref.shape[0])


def shared_kernel(normed_ref, gate_ref, up_ref, down_ref, gain_ref, out_ref, gain_out):
    normed = normed_ref[...]
    gate_part = dot(normed, gate_ref[...])
    up_part = dot(normed, up_ref[...])
    hidden = (gate_part / (1.0 + jnp.exp(-gate_part)) * up_part).astype(bf16)
    out_ref[...] = dot(hidden, down_ref[...])
    gain_out[...] = gain_ref[...]


def final_kernel(returned_ref, aux_ref, extra_ref, shared_ref, gain_ref, out_ref):
    seqs, new, features = out_ref.shape
    routed = fetched_sum(returned_ref, aux_ref, seqs * new) + extra_ref[...]
    summed = routed + shared_ref[...]
    mixed = summed * lax.rsqrt(jnp.mean(summed * summed, axis=-1, keepdims=True) + EPS) * gain_ref[...]
    mixed = jnp.where(aux_ref[: seqs * new, 2:3] > 0.0, mixed, 0.0)
    for s in range(seqs):
        out_ref[s] = mixed[s * new : (s + 1) * new].astype(bf16)


VMEM = pl.BlockSpec(memory_space=pltpu.VMEM)
SMEM = pl.BlockSpec(memory_space=pltpu.SMEM)
HBM = pl.BlockSpec(memory_space=pltpu.HBM)


def limit(mib):
    return pltpu.CompilerParams(vmem_limit_bytes=mib * 1024 * 1024)


def per_device(
    tokens, lengths, routes, gates, norm_gain, expert_gate, expert_up, expert_down,
    shared_gate, shared_up, shared_down, out_gain,
):
    seqs, new, features = tokens.shape
    rows = seqs * new
    top = routes.shape[2]
    devices = lax.axis_size("ep")
    chips = devices // 2
    slots_all = chips * SLOTS
    pairs = rows * top
    core = jnp.full((8, 128), (lax.axis_index("ep") & 1).astype(i32))
    groups = [[2 * c + k for c in range(chips)] for k in range(2)]
    sibling = functools.partial(lax.ppermute, axis_name="ep", perm=[(d, d ^ 1) for d in range(devices)])

    def dispatch(base):
        return pl.pallas_call(
            functools.partial(dispatch_kernel, base=base),
            out_shape=(
                pltpu.HBM((slots_all, features + LABELS), bf16),
                jax.ShapeDtypeStruct((pairs, 128), f32),
                jax.ShapeDtypeStruct((rows, features), bf16),
            ),
            in_specs=[SMEM] + [VMEM] * 4,
            out_specs=(HBM, VMEM, VMEM),
            scratch_shapes=[
                pltpu.VMEM((rows, features), f32),
                pltpu.VMEM((rows, top), i32),
                pltpu.VMEM((rows, top), f32),
                pltpu.VMEM((slots_all, features + LABELS), bf16),
                pltpu.SemaphoreType.DMA((CHUNKS,)),
            ],
            compiler_params=limit(12),
            name="dispatch",
        )(lengths, tokens, routes, gates, norm_gain.reshape(1, features))

    def exchange(values):
        width = values.shape[1]
        return lax.all_to_all(
            values.reshape(chips, SLOTS, width), "ep", split_axis=0, concat_axis=0,
            axis_index_groups=groups, tiled=True,
        ).reshape(slots_all, width)

    def experts(arrived, weights):
        return pl.pallas_call(
            expert_kernel,
            out_shape=(
                pltpu.HBM((slots_all, features), bf16),
                jax.ShapeDtypeStruct((1,), i32),
            ),
            in_specs=[VMEM, VMEM, HBM, VMEM, HBM, VMEM, HBM, HBM],
            out_specs=(HBM, SMEM),
            scratch_shapes=[
                pltpu.VMEM((slots_all + 256, features), bf16),
                pltpu.VMEM((slots_all + 256, features), bf16),
                pltpu.VMEM((slots_all, features), bf16),
                *[pltpu.VMEM(w.shape, bf16) for w in (*own, expert_down)],
                pltpu.SemaphoreType.DMA((CHUNKS,)),
                pltpu.SemaphoreType.DMA((1 + 3 * expert_gate.shape[0],)),
            ],
            compiler_params=limit(24),
            name="experts",
        )(core, arrived, *weights)

    own = (expert_gate, expert_up, expert_down)
    send, aux, normed = dispatch(0)
    weights = [w for v in own for w in (v, sibling(v))]

    arrived = exchange(send)
    replies, flag = experts(arrived, weights)
    shared, gain = pl.pallas_call(
        shared_kernel,
        out_shape=(
            jax.ShapeDtypeStruct((rows, features), f32),
            jax.ShapeDtypeStruct((1, features), f32),
        ),
        in_specs=[VMEM] * 5,
        out_specs=(VMEM, VMEM),
        compiler_params=limit(8),
        name="shared",
    )(normed, shared_gate, shared_up, shared_down, out_gain.reshape(1, features))
    flags = flag + sibling(flag)
    returned = exchange(replies)
    flags, returned = lax.optimization_barrier((flags, returned))

    def second_round():
        send, aux, _ = dispatch(SLOTS)
        again = lax.optimization_barrier((send, *own))
        weights = [w for v in again[1:] for w in (v, sibling(v))]
        replies, _ = experts(exchange(again[0]), weights)
        return pl.pallas_call(
            combine_kernel,
            out_shape=jax.ShapeDtypeStruct((rows, features), f32),
            in_specs=[VMEM] * 2,
            out_specs=VMEM,
            compiler_params=limit(8),
            name="combine",
        )(exchange(replies), aux)

    extra = lax.cond(flags[0] > 0, second_round, lambda: jnp.zeros((rows, features), f32))
    return pl.pallas_call(
        final_kernel,
        out_shape=jax.ShapeDtypeStruct(tokens.shape, bf16),
        in_specs=[VMEM] * 5,
        out_specs=VMEM,
        compiler_params=limit(8),
        name="final",
    )(returned, aux, extra, shared, gain)


def solution(mesh):
    placed = (
        P("ep", None, None),
        P("ep"),
        P("ep", None, None),
        P("ep", None, None),
        P(),
        P("ep", None, None),
        P("ep", None, None),
        P("ep", None, None),
        P(),
        P(),
        P(),
        P(),
    )
    return jax.shard_map(
        per_device, mesh=mesh, in_specs=placed, out_specs=P("ep", None, None), check_vma=False
    )
```

```python
import functools

import jax
import jax.numpy as jnp
from jax import lax
from jax.experimental import pallas as pl
from jax.experimental.pallas import tpu as pltpu
from jax.sharding import PartitionSpec as P

EPS = 1e-06
SLOTS = 8
LABELS = 128
CHUNKS = 4
FLAG_LANE = 64

f32 = jnp.float32
bf16 = jnp.bfloat16
i32 = jnp.int32


def iota(shape, dim):
    return lax.broadcasted_iota(i32, shape, dim)


def dot(a, b):
    return jnp.dot(a, b, preferred_element_type=f32)


def one_hot(mask):
    return jnp.where(mask, 1.0, 0.0).astype(bf16)


def spread(columns, top):
    rows = columns.shape[0]
    return jnp.concatenate(
        [jnp.broadcast_to(columns[:, k : k + 1], (rows, 128)) for k in range(top)], axis=0
    )


def dispatch_kernel(len_ref, tok, rt, gt, gain_ref, send_hbm, aux_ref, normed_ref, x_s, r_s, g_s, send_s, sems, *, base):
    seqs, new, features = tok.shape
    rows = seqs * new
    top = rt.shape[2]
    pairs = rows * top
    slots_all = send_hbm.shape[0]
    for i in range(seqs):
        x_s[i * new : (i + 1) * new, :] = tok[i].astype(f32)
        r_s[i * new : (i + 1) * new, :] = rt[i]
        g_s[i * new : (i + 1) * new, :] = gt[i]

    wide = x_s[...]
    normed = wide * lax.rsqrt(jnp.mean(wide * wide, axis=-1, keepdims=True) + EPS) * gain_ref[...]
    normed = normed.astype(bf16)
    normed_ref[...] = normed

    token = iota((rows, 128), 0)
    length = jnp.zeros((rows, 128), i32)
    for s in range(seqs):
        length = jnp.where(token // new == s, len_ref[s], length)
    live = jnp.concatenate([jnp.where(token % new < length, 1, 0)] * top, axis=0) > 0
    expert = spread(r_s[...], top)
    gate = spread(g_s[...], top)

    chip = jnp.where(live, expert >> 2, -1).astype(f32)
    local = (expert & 3).astype(f32)
    i0, i1 = iota((pairs, pairs), 0), iota((pairs, pairs), 1)
    chip_row = jnp.sum(jnp.where(i0 == i1, chip, 0.0), axis=0, keepdims=True)
    equal = chip == chip_row
    pos_row = jnp.sum(jnp.where(equal & (i0 < i1), 1.0, 0.0), axis=0, keepdims=True).astype(i32)
    pos_col = jnp.sum(jnp.where(equal & (i1 < i0), 1.0, 0.0), axis=1, keepdims=True).astype(i32)

    def placed(where_to, pos):
        chip_i = where_to.astype(i32)
        slot = pos - base
        mine = (chip_i >= 0) & (slot >= 0) & (slot < SLOTS)
        return jnp.where(mine, chip_i * SLOTS + slot, -1)

    target_row = placed(chip_row, pos_row)
    target_col = placed(chip, jnp.broadcast_to(pos_col, chip.shape))
    over = jnp.where((chip_row >= 0.0) & (pos_row >= base + SLOTS), 1.0, 0.0)
    over = jnp.sum(over, axis=1, keepdims=True)

    lane = iota((pairs, LABELS), 1)
    labels = jnp.where(lane == 0, local + 1.0, 0.0).astype(bf16)
    alive = jnp.where(live, 1.0, 0.0)
    aux_ref[...] = jnp.where(
        lane == 0, target_col.astype(f32), jnp.where(lane == 1, gate, jnp.where(lane == 2, alive, 0.0))
    )
    copies = jnp.concatenate([normed] * top, axis=0)
    step = slots_all // CHUNKS
    flag_lane = iota((step, LABELS), 1) == FLAG_LANE
    outward = []
    for c in range(CHUNKS):
        at = c * step
        picks = one_hot(iota((step, pairs), 0) + at == target_row)
        send_s[at : at + step, :features] = dot(picks, copies).astype(bf16)
        marks = jnp.where(flag_lane, over, dot(picks, labels))
        send_s[at : at + step, features:] = marks.astype(bf16)
        part = pl.ds(at, step)
        outward.append(pltpu.make_async_copy(send_s.at[part], send_hbm.at[part], sems.at[c]))
        outward[-1].start()
    for copy in outward:
        copy.wait()


def expert_kernel(
    core_ref, arrived_ref, gate_hbm, gate_sib, up_hbm, up_sib, down_hbm, down_sib_hbm,
    reply_hbm, flag_ref, x_s, o_s, reply_s, gate_own, up_own, down_own, down_sib, sems, weight_sems,
):
    core = jnp.concatenate([core_ref[0:1, :]] * (arrived_ref.shape[0] // 128), axis=1)
    own = gate_own.shape[0]
    parts = [(down_sib_hbm, down_sib)]
    for e in range(own):
        parts += [
            (gate_hbm.at[e], gate_own.at[e]), (up_hbm.at[e], up_own.at[e]), (down_hbm.at[e], down_own.at[e])
        ]
    inward = [
        pltpu.make_async_copy(source, target, weight_sems.at[i])
        for i, (source, target) in enumerate(parts)
    ]
    for copy in inward:
        copy.start()
    features = reply_hbm.shape[1]
    slots_all = arrived_ref.shape[0]

    r8, l8 = iota((8, LABELS), 0), iota((8, LABELS), 1)
    wanted = one_hot(((r8 == 0) & (l8 == 0)) | ((r8 == 1) & (l8 == FLAG_LANE)))
    found = lax.dot_general(
        wanted, arrived_ref[:, features:], (((1,), (1,)), ((), ())), preferred_element_type=f32
    )
    flag_ref[0] = jnp.where(jnp.sum(found[1:2]) > 0.0, 1, 0)
    ids = found[0:1].astype(i32)
    which = jnp.where(ids > 0, (ids - 1 + own * core + own) & (2 * own - 1), -1)
    hot = one_hot(iota((8, slots_all), 0) == which)
    earlier = one_hot(iota((slots_all, slots_all), 0) < iota((slots_all, slots_all), 1))
    rank = dot(hot, earlier).astype(i32)
    place = jnp.full((1, slots_all), -1, i32)
    start = jnp.int32(0)
    spans = []
    for j in range(2 * own):
        count = jnp.sum(jnp.where(which == j, 1.0, 0.0)).astype(i32)
        place = jnp.where(which == j, rank[j : j + 1] + start, place)
        spans.append((start, count))
        start = start + ((count + 15) // 16) * 16
    total = start
    most = slots_all + 128

    blocks = (total + 127) // 128

    def gather(b, carry):
        at = pl.multiple_of(b * 128, 128)
        picks = one_hot(iota((128, slots_all), 0) + at == place)
        x_s[pl.ds(at, 128), :] = dot(picks, arrived_ref[:, :features]).astype(bf16)
        return carry

    lax.fori_loop(0, blocks, gather, 0)
    x_s[pl.ds(pl.multiple_of(blocks * 128, 128), 128), :] = jnp.zeros((128, features), bf16)
    o_s[:256, :] = jnp.zeros((256, features), bf16)

    @pl.when(total > 256)
    def _():
        o_s[256:most, :] = jnp.zeros((most - 256, features), bf16)

    def run(items, size):
        rows = [x_s[pl.ds(pl.multiple_of(at, 16), size), :] for at, _, _ in items]
        gates = [dot(x, w[0][e]) for x, (_, w, e) in zip(rows, items)]
        ups = [dot(x, w[1][e]) for x, (_, w, e) in zip(rows, items)]
        mids = [(g / (1.0 + jnp.exp(-g)) * u).astype(bf16) for g, u in zip(gates, ups)]
        outs = [dot(h, w[2][e]).astype(bf16) for h, (_, w, e) in zip(mids, items)]
        for out, (at, _, _) in zip(outs, items):
            o_s[pl.ds(pl.multiple_of(at, 16), size), :] = out

    for lowest, w in ((0, (gate_sib, up_sib, down_sib)), (own, (gate_own, up_own, down_own))):
        for copy in inward[:1] if lowest == 0 else inward[1:]:
            copy.wait()
        group = spans[lowest : lowest + own]
        largest = functools.reduce(jnp.maximum, [count for _, count in group])

        @pl.when(largest <= 64)
        def _(group=group, w=w):
            run([(begin, w, e) for e, (begin, _) in enumerate(group)], 64)

        @pl.when(largest > 64)
        def _(group=group, w=w):
            for e, (begin, count) in enumerate(group):

                def body(b, carry, begin=begin, e=e):
                    run([(begin + b * 128, w, e)], 128)
                    return carry

                lax.fori_loop(0, (count + 127) // 128, body, 0)

    place_f = place.astype(f32)

    def scatter(depth):
        step = slots_all // CHUNKS
        outward = []
        for c in range(CHUNKS):
            at = c * step
            same = iota((step, slots_all), 0) + at == iota((step, slots_all), 1)
            column = jnp.sum(jnp.where(same, place_f, 0.0), axis=1, keepdims=True).astype(i32)
            picks = one_hot(iota((step, depth), 1) == column)
            reply_s[at : at + step, :] = dot(picks, o_s[:depth, :]).astype(bf16)
            part = pl.ds(at, step)
            outward.append(pltpu.make_async_copy(reply_s.at[part], reply_hbm.at[part], sems.at[c]))
            outward[-1].start()
        for copy in outward:
            copy.wait()

    @pl.when(total <= 256)
    def _():
        scatter(256)

    @pl.when(total > 256)
    def _():
        scatter(most)


def fetched_sum(returned_ref, aux_ref, rows):
    pairs = aux_ref.shape[0]
    target = aux_ref[:, 0:1].astype(i32)
    picks = one_hot(iota((pairs, returned_ref.shape[0]), 1) == target)
    weighted = dot(picks, returned_ref[...]) * aux_ref[:, 1:2]
    total = weighted[:rows]
    for k in range(rows, pairs, rows):
        total = total + weighted[k : k + rows]
    return total


def combine_kernel(returned_ref, aux_ref, out_ref):
    out_ref[...] = fetched_sum(returned_ref, aux_ref, out_ref.shape[0])


def shared_kernel(normed_ref, gate_ref, up_ref, down_ref, gain_ref, out_ref, gain_out):
    normed = normed_ref[...]
    gate_part = dot(normed, gate_ref[...])
    up_part = dot(normed, up_ref[...])
    hidden = (gate_part / (1.0 + jnp.exp(-gate_part)) * up_part).astype(bf16)
    out_ref[...] = dot(hidden, down_ref[...])
    gain_out[...] = gain_ref[...]


def final_kernel(returned_ref, aux_ref, extra_ref, shared_ref, gain_ref, out_ref):
    seqs, new, features = out_ref.shape
    routed = fetched_sum(returned_ref, aux_ref, seqs * new) + extra_ref[...]
    summed = routed + shared_ref[...]
    mixed = summed * lax.rsqrt(jnp.mean(summed * summed, axis=-1, keepdims=True) + EPS) * gain_ref[...]
    mixed = jnp.where(aux_ref[: seqs * new, 2:3] > 0.0, mixed, 0.0)
    for s in range(seqs):
        out_ref[s] = mixed[s * new : (s + 1) * new].astype(bf16)


VMEM = pl.BlockSpec(memory_space=pltpu.VMEM)
SMEM = pl.BlockSpec(memory_space=pltpu.SMEM)
HBM = pl.BlockSpec(memory_space=pltpu.HBM)


def limit(mib):
    return pltpu.CompilerParams(vmem_limit_bytes=mib * 1024 * 1024)


def per_device(
    tokens, lengths, routes, gates, norm_gain, expert_gate, expert_up, expert_down,
    shared_gate, shared_up, shared_down, out_gain,
):
    seqs, new, features = tokens.shape
    rows = seqs * new
    top = routes.shape[2]
    devices = lax.axis_size("ep")
    chips = devices // 2
    slots_all = chips * SLOTS
    pairs = rows * top
    core = jnp.full((8, 128), (lax.axis_index("ep") & 1).astype(i32))
    groups = [[2 * c + k for c in range(chips)] for k in range(2)]
    sibling = functools.partial(lax.ppermute, axis_name="ep", perm=[(d, d ^ 1) for d in range(devices)])

    def dispatch(base):
        return pl.pallas_call(
            functools.partial(dispatch_kernel, base=base),
            out_shape=(
                pltpu.HBM((slots_all, features + LABELS), bf16),
                jax.ShapeDtypeStruct((pairs, 128), f32),
                jax.ShapeDtypeStruct((rows, features), bf16),
            ),
            in_specs=[SMEM] + [VMEM] * 4,
            out_specs=(HBM, VMEM, VMEM),
            scratch_shapes=[
                pltpu.VMEM((rows, features), f32),
                pltpu.VMEM((rows, top), i32),
                pltpu.VMEM((rows, top), f32),
                pltpu.VMEM((slots_all, features + LABELS), bf16),
                pltpu.SemaphoreType.DMA((CHUNKS,)),
            ],
            compiler_params=limit(12),
            name="dispatch",
        )(lengths, tokens, routes, gates, norm_gain.reshape(1, features))

    def exchange(values):
        width = values.shape[1]
        return lax.all_to_all(
            values.reshape(chips, SLOTS, width), "ep", split_axis=0, concat_axis=0,
            axis_index_groups=groups, tiled=True,
        ).reshape(slots_all, width)

    def experts(arrived, weights):
        return pl.pallas_call(
            expert_kernel,
            out_shape=(
                pltpu.HBM((slots_all, features), bf16),
                jax.ShapeDtypeStruct((1,), i32),
            ),
            in_specs=[VMEM, VMEM, HBM, VMEM, HBM, VMEM, HBM, HBM],
            out_specs=(HBM, SMEM),
            scratch_shapes=[
                pltpu.VMEM((slots_all + 256, features), bf16),
                pltpu.VMEM((slots_all + 256, features), bf16),
                pltpu.VMEM((slots_all, features), bf16),
                *[pltpu.VMEM(w.shape, bf16) for w in (*own, expert_down)],
                pltpu.SemaphoreType.DMA((CHUNKS,)),
                pltpu.SemaphoreType.DMA((1 + 3 * expert_gate.shape[0],)),
            ],
            compiler_params=limit(24),
            name="experts",
        )(core, arrived, *weights)

    own = (expert_gate, expert_up, expert_down)
    send, aux, normed = dispatch(0)
    weights = [w for v in own for w in (v, sibling(v))]

    arrived = exchange(send)
    replies, flag = experts(arrived, weights)
    shared, gain = pl.pallas_call(
        shared_kernel,
        out_shape=(
            jax.ShapeDtypeStruct((rows, features), f32),
            jax.ShapeDtypeStruct((1, features), f32),
        ),
        in_specs=[VMEM] * 5,
        out_specs=(VMEM, VMEM),
        compiler_params=limit(8),
        name="shared",
    )(normed, shared_gate, shared_up, shared_down, out_gain.reshape(1, features))
    flags = flag + sibling(flag)
    returned = exchange(replies)
    flags, returned = lax.optimization_barrier((flags, returned))

    def second_round():
        send, aux, _ = dispatch(SLOTS)
        again = lax.optimization_barrier((send, *own))
        weights = [w for v in again[1:] for w in (v, sibling(v))]
        replies, _ = experts(exchange(again[0]), weights)
        return pl.pallas_call(
            combine_kernel,
            out_shape=jax.ShapeDtypeStruct((rows, features), f32),
            in_specs=[VMEM] * 2,
            out_specs=VMEM,
            compiler_params=limit(8),
            name="combine",
        )(exchange(replies), aux)

    extra = lax.cond(flags[0] > 0, second_round, lambda: jnp.zeros((rows, features), f32))
    return pl.pallas_call(
        final_kernel,
        out_shape=jax.ShapeDtypeStruct(tokens.shape, bf16),
        in_specs=[VMEM] * 5,
        out_specs=VMEM,
        compiler_params=limit(8),
        name="final",
    )(returned, aux, extra, shared, gain)


def solution(mesh):
    placed = (
        P("ep", None, None),
        P("ep"),
        P("ep", None, None),
        P("ep", None, None),
        P(),
        P("ep", None, None),
        P("ep", None, None),
        P("ep", None, None),
        P(),
        P(),
        P(),
        P(),
    )
    return jax.shard_map(
        per_device, mesh=mesh, in_specs=placed, out_specs=P("ep", None, None), check_vma=False
    )
```

```python
import functools

import jax
import jax.numpy as jnp
from jax import lax
from jax.experimental import pallas as pl
from jax.experimental.pallas import tpu as pltpu
from jax.sharding import PartitionSpec as P

EPS = 1e-06
SLOTS = 8
LABELS = 128
CHUNKS = 2
FLAG_LANE = 64

f32 = jnp.float32
bf16 = jnp.bfloat16
i32 = jnp.int32


def iota(shape, dim):
    return lax.broadcasted_iota(i32, shape, dim)


def dot(a, b):
    return jnp.dot(a, b, preferred_element_type=f32)


def one_hot(mask):
    return jnp.where(mask, 1.0, 0.0).astype(bf16)


def spread(columns, top):
    rows = columns.shape[0]
    return jnp.concatenate(
        [jnp.broadcast_to(columns[:, k : k + 1], (rows, 128)) for k in range(top)], axis=0
    )


def dispatch_kernel(len_ref, tok, rt, gt, gain_ref, send_hbm, aux_ref, normed_ref, x_s, r_s, g_s, send_s, sems, *, base):
    seqs, new, features = tok.shape
    rows = seqs * new
    top = rt.shape[2]
    pairs = rows * top
    slots_all = send_hbm.shape[0]
    for i in range(seqs):
        x_s[i * new : (i + 1) * new, :] = tok[i].astype(f32)
        r_s[i * new : (i + 1) * new, :] = rt[i]
        g_s[i * new : (i + 1) * new, :] = gt[i]

    wide = x_s[...]
    normed = wide * lax.rsqrt(jnp.mean(wide * wide, axis=-1, keepdims=True) + EPS) * gain_ref[...]
    normed = normed.astype(bf16)
    normed_ref[...] = normed

    token = iota((rows, 128), 0)
    length = jnp.zeros((rows, 128), i32)
    for s in range(seqs):
        length = jnp.where(token // new == s, len_ref[s], length)
    live = jnp.concatenate([jnp.where(token % new < length, 1, 0)] * top, axis=0) > 0
    expert = spread(r_s[...], top)
    gate = spread(g_s[...], top)

    chip = jnp.where(live, expert >> 2, -1).astype(f32)
    local = (expert & 3).astype(f32)
    i0, i1 = iota((pairs, pairs), 0), iota((pairs, pairs), 1)
    chip_row = jnp.sum(jnp.where(i0 == i1, chip, 0.0), axis=0, keepdims=True)
    equal = chip == chip_row
    pos_row = jnp.sum(jnp.where(equal & (i0 < i1), 1.0, 0.0), axis=0, keepdims=True).astype(i32)
    pos_col = jnp.sum(jnp.where(equal & (i1 < i0), 1.0, 0.0), axis=1, keepdims=True).astype(i32)

    def placed(where_to, pos):
        chip_i = where_to.astype(i32)
        slot = pos - base
        mine = (chip_i >= 0) & (slot >= 0) & (slot < SLOTS)
        return jnp.where(mine, chip_i * SLOTS + slot, -1)

    target_row = placed(chip_row, pos_row)
    target_col = placed(chip, jnp.broadcast_to(pos_col, chip.shape))
    over = jnp.where((chip_row >= 0.0) & (pos_row >= base + SLOTS), 1.0, 0.0)
    over = jnp.sum(over, axis=1, keepdims=True)

    lane = iota((pairs, LABELS), 1)
    labels = jnp.where(lane == 0, local + 1.0, 0.0).astype(bf16)
    alive = jnp.where(live, 1.0, 0.0)
    aux_ref[...] = jnp.where(
        lane == 0, target_col.astype(f32), jnp.where(lane == 1, gate, jnp.where(lane == 2, alive, 0.0))
    )
    copies = jnp.concatenate([normed] * top, axis=0)
    step = slots_all // CHUNKS
    flag_lane = iota((step, LABELS), 1) == FLAG_LANE
    outward = []
    for c in range(CHUNKS):
        at = c * step
        picks = one_hot(iota((step, pairs), 0) + at == target_row)
        send_s[at : at + step, :features] = dot(picks, copies).astype(bf16)
        marks = jnp.where(flag_lane, over, dot(picks, labels))
        send_s[at : at + step, features:] = marks.astype(bf16)
        part = pl.ds(at, step)
        outward.append(pltpu.make_async_copy(send_s.at[part], send_hbm.at[part], sems.at[c]))
        outward[-1].start()
    for copy in outward:
        copy.wait()


def expert_kernel(
    core_ref, arrived_ref, gate_hbm, gate_sib, up_hbm, up_sib, down_hbm, down_sib_hbm,
    reply_hbm, flag_ref, x_s, o_s, reply_s, gate_own, up_own, down_own, down_sib, sems, weight_sems,
):
    core = jnp.concatenate([core_ref[0:1, :]] * (arrived_ref.shape[0] // 128), axis=1)
    own = gate_own.shape[0]
    parts = [(down_sib_hbm, down_sib)]
    for e in range(own):
        parts += [
            (gate_hbm.at[e], gate_own.at[e]), (up_hbm.at[e], up_own.at[e]), (down_hbm.at[e], down_own.at[e])
        ]
    inward = [
        pltpu.make_async_copy(source, target, weight_sems.at[i])
        for i, (source, target) in enumerate(parts)
    ]
    for copy in inward:
        copy.start()
    features = reply_hbm.shape[1]
    slots_all = arrived_ref.shape[0]

    r8, l8 = iota((8, LABELS), 0), iota((8, LABELS), 1)
    wanted = one_hot(((r8 == 0) & (l8 == 0)) | ((r8 == 1) & (l8 == FLAG_LANE)))
    found = lax.dot_general(
        wanted, arrived_ref[:, features:], (((1,), (1,)), ((), ())), preferred_element_type=f32
    )
    flag_ref[0] = jnp.where(jnp.sum(found[1:2]) > 0.0, 1, 0)
    ids = found[0:1].astype(i32)
    which = jnp.where(ids > 0, (ids - 1 + own * core + own) & (2 * own - 1), -1)
    hot = one_hot(iota((8, slots_all), 0) == which)
    earlier = one_hot(iota((slots_all, slots_all), 0) < iota((slots_all, slots_all), 1))
    rank = dot(hot, earlier).astype(i32)
    place = jnp.full((1, slots_all), -1, i32)
    start = jnp.int32(0)
    spans = []
    for j in range(2 * own):
        count = jnp.sum(jnp.where(which == j, 1.0, 0.0)).astype(i32)
        place = jnp.where(which == j, rank[j : j + 1] + start, place)
        spans.append((start, count))
        start = start + ((count + 15) // 16) * 16
    total = start
    most = slots_all + 128

    blocks = (total + 127) // 128

    def gather(b, carry):
        at = pl.multiple_of(b * 128, 128)
        picks = one_hot(iota((128, slots_all), 0) + at == place)
        x_s[pl.ds(at, 128), :] = dot(picks, arrived_ref[:, :features]).astype(bf16)
        return carry

    lax.fori_loop(0, blocks, gather, 0)
    x_s[pl.ds(pl.multiple_of(blocks * 128, 128), 128), :] = jnp.zeros((128, features), bf16)
    o_s[:256, :] = jnp.zeros((256, features), bf16)

    @pl.when(total > 256)
    def _():
        o_s[256:most, :] = jnp.zeros((most - 256, features), bf16)

    def run(items, size):
        rows = [x_s[pl.ds(pl.multiple_of(at, 16), size), :] for at, _, _ in items]
        gates = [dot(x, w[0][e]) for x, (_, w, e) in zip(rows, items)]
        ups = [dot(x, w[1][e]) for x, (_, w, e) in zip(rows, items)]
        mids = [(g / (1.0 + jnp.exp(-g)) * u).astype(bf16) for g, u in zip(gates, ups)]
        outs = [dot(h, w[2][e]).astype(bf16) for h, (_, w, e) in zip(mids, items)]
        for out, (at, _, _) in zip(outs, items):
            o_s[pl.ds(pl.multiple_of(at, 16), size), :] = out

    for lowest, w in ((0, (gate_sib, up_sib, down_sib)), (own, (gate_own, up_own, down_own))):
        for copy in inward[:1] if lowest == 0 else inward[1:]:
            copy.wait()
        group = spans[lowest : lowest + own]
        largest = functools.reduce(jnp.maximum, [count for _, count in group])

        @pl.when(largest <= 64)
        def _(group=group, w=w):
            run([(begin, w, e) for e, (begin, _) in enumerate(group)], 64)

        @pl.when(largest > 64)
        def _(group=group, w=w):
            for e, (begin, count) in enumerate(group):

                def body(b, carry, begin=begin, e=e):
                    run([(begin + b * 128, w, e)], 128)
                    return carry

                lax.fori_loop(0, (count + 127) // 128, body, 0)

    place_f = place.astype(f32)

    def scatter(depth):
        step = slots_all // CHUNKS
        outward = []
        for c in range(CHUNKS):
            at = c * step
            same = iota((step, slots_all), 0) + at == iota((step, slots_all), 1)
            column = jnp.sum(jnp.where(same, place_f, 0.0), axis=1, keepdims=True).astype(i32)
            picks = one_hot(iota((step, depth), 1) == column)
            reply_s[at : at + step, :] = dot(picks, o_s[:depth, :]).astype(bf16)
            part = pl.ds(at, step)
            outward.append(pltpu.make_async_copy(reply_s.at[part], reply_hbm.at[part], sems.at[c]))
            outward[-1].start()
        for copy in outward:
            copy.wait()

    @pl.when(total <= 256)
    def _():
        scatter(256)

    @pl.when(total > 256)
    def _():
        scatter(most)


def fetched_sum(returned_ref, aux_ref, rows):
    pairs = aux_ref.shape[0]
    target = aux_ref[:, 0:1].astype(i32)
    picks = one_hot(iota((pairs, returned_ref.shape[0]), 1) == target)
    weighted = dot(picks, returned_ref[...]) * aux_ref[:, 1:2]
    total = weighted[:rows]
    for k in range(rows, pairs, rows):
        total = total + weighted[k : k + rows]
    return total


def combine_kernel(returned_ref, aux_ref, out_ref):
    out_ref[...] = fetched_sum(returned_ref, aux_ref, out_ref.shape[0])


def shared_kernel(normed_ref, gate_ref, up_ref, down_ref, gain_ref, out_ref, gain_out):
    normed = normed_ref[...]
    gate_part = dot(normed, gate_ref[...])
    up_part = dot(normed, up_ref[...])
    hidden = (gate_part / (1.0 + jnp.exp(-gate_part)) * up_part).astype(bf16)
    out_ref[...] = dot(hidden, down_ref[...])
    gain_out[...] = gain_ref[...]


def final_kernel(returned_ref, aux_ref, extra_ref, shared_ref, gain_ref, out_ref):
    seqs, new, features = out_ref.shape
    routed = fetched_sum(returned_ref, aux_ref, seqs * new) + extra_ref[...]
    summed = routed + shared_ref[...]
    mixed = summed * lax.rsqrt(jnp.mean(summed * summed, axis=-1, keepdims=True) + EPS) * gain_ref[...]
    mixed = jnp.where(aux_ref[: seqs * new, 2:3] > 0.0, mixed, 0.0)
    for s in range(seqs):
        out_ref[s] = mixed[s * new : (s + 1) * new].astype(bf16)


VMEM = pl.BlockSpec(memory_space=pltpu.VMEM)
SMEM = pl.BlockSpec(memory_space=pltpu.SMEM)
HBM = pl.BlockSpec(memory_space=pltpu.HBM)


def limit(mib):
    return pltpu.CompilerParams(vmem_limit_bytes=mib * 1024 * 1024)


def per_device(
    tokens, lengths, routes, gates, norm_gain, expert_gate, expert_up, expert_down,
    shared_gate, shared_up, shared_down, out_gain,
):
    seqs, new, features = tokens.shape
    rows = seqs * new
    top = routes.shape[2]
    devices = lax.axis_size("ep")
    chips = devices // 2
    slots_all = chips * SLOTS
    pairs = rows * top
    core = jnp.full((8, 128), (lax.axis_index("ep") & 1).astype(i32))
    groups = [[2 * c + k for c in range(chips)] for k in range(2)]
    sibling = functools.partial(lax.ppermute, axis_name="ep", perm=[(d, d ^ 1) for d in range(devices)])

    def dispatch(base):
        return pl.pallas_call(
            functools.partial(dispatch_kernel, base=base),
            out_shape=(
                pltpu.HBM((slots_all, features + LABELS), bf16),
                jax.ShapeDtypeStruct((pairs, 128), f32),
                jax.ShapeDtypeStruct((rows, features), bf16),
            ),
            in_specs=[SMEM] + [VMEM] * 4,
            out_specs=(HBM, VMEM, VMEM),
            scratch_shapes=[
                pltpu.VMEM((rows, features), f32),
                pltpu.VMEM((rows, top), i32),
                pltpu.VMEM((rows, top), f32),
                pltpu.VMEM((slots_all, features + LABELS), bf16),
                pltpu.SemaphoreType.DMA((CHUNKS,)),
            ],
            compiler_params=limit(12),
            name="dispatch",
        )(lengths, tokens, routes, gates, norm_gain.reshape(1, features))

    def exchange(values):
        width = values.shape[1]
        return lax.all_to_all(
            values.reshape(chips, SLOTS, width), "ep", split_axis=0, concat_axis=0,
            axis_index_groups=groups, tiled=True,
        ).reshape(slots_all, width)

    def experts(arrived, weights):
        return pl.pallas_call(
            expert_kernel,
            out_shape=(
                pltpu.HBM((slots_all, features), bf16),
                jax.ShapeDtypeStruct((1,), i32),
            ),
            in_specs=[VMEM, VMEM, HBM, VMEM, HBM, VMEM, HBM, HBM],
            out_specs=(HBM, SMEM),
            scratch_shapes=[
                pltpu.VMEM((slots_all + 256, features), bf16),
                pltpu.VMEM((slots_all + 256, features), bf16),
                pltpu.VMEM((slots_all, features), bf16),
                *[pltpu.VMEM(w.shape, bf16) for w in (*own, expert_down)],
                pltpu.SemaphoreType.DMA((CHUNKS,)),
                pltpu.SemaphoreType.DMA((1 + 3 * expert_gate.shape[0],)),
            ],
            compiler_params=limit(24),
            name="experts",
        )(core, arrived, *weights)

    own = (expert_gate, expert_up, expert_down)
    send, aux, normed = dispatch(0)
    weights = [w for v in own for w in (v, sibling(v))]

    arrived = exchange(send)
    replies, flag = experts(arrived, weights)
    shared, gain = pl.pallas_call(
        shared_kernel,
        out_shape=(
            jax.ShapeDtypeStruct((rows, features), f32),
            jax.ShapeDtypeStruct((1, features), f32),
        ),
        in_specs=[VMEM] * 5,
        out_specs=(VMEM, VMEM),
        compiler_params=limit(8),
        name="shared",
    )(normed, shared_gate, shared_up, shared_down, out_gain.reshape(1, features))
    flags = flag + sibling(flag)
    returned = exchange(replies)
    flags, returned = lax.optimization_barrier((flags, returned))

    def second_round():
        send, aux, _ = dispatch(SLOTS)
        again = lax.optimization_barrier((send, *own))
        weights = [w for v in again[1:] for w in (v, sibling(v))]
        replies, _ = experts(exchange(again[0]), weights)
        return pl.pallas_call(
            combine_kernel,
            out_shape=jax.ShapeDtypeStruct((rows, features), f32),
            in_specs=[VMEM] * 2,
            out_specs=VMEM,
            compiler_params=limit(8),
            name="combine",
        )(exchange(replies), aux)

    extra = lax.cond(flags[0] > 0, second_round, lambda: jnp.zeros((rows, features), f32))
    return pl.pallas_call(
        final_kernel,
        out_shape=jax.ShapeDtypeStruct(tokens.shape, bf16),
        in_specs=[VMEM] * 5,
        out_specs=VMEM,
        compiler_params=limit(8),
        name="final",
    )(returned, aux, extra, shared, gain)


def solution(mesh):
    placed = (
        P("ep", None, None),
        P("ep"),
        P("ep", None, None),
        P("ep", None, None),
        P(),
        P("ep", None, None),
        P("ep", None, None),
        P("ep", None, None),
        P(),
        P(),
        P(),
        P(),
    )
    return jax.shard_map(
        per_device, mesh=mesh, in_specs=placed, out_specs=P("ep", None, None), check_vma=False
    )
```
